32 devices in a mesh: sp: 8 (over z, y), tp: 4 (over x, core).
Axes of the slice: x: 2, y: 2, z: 4, core: 2. Of those that a mesh axis runs over, the one named last changes fastest.
Arguments:
- hidden_in: bfloat16 [6144, 4096], P('sp', 'tp'), may hold values from -16 to 16
- norm_gain: bfloat16 [2, 4096], P(None, 'tp'), may hold values from 0.099609375 to 1.8984375
- value_proj: bfloat16 [2, 4096, 1024], P(None, 'tp', 'sp'), may hold values from -0.09375 to 0.09375
- gate_proj: bfloat16 [2, 4096, 1024], P(None, 'tp', 'sp'), may hold values from -0.09375 to 0.09375
- conv_taps: bfloat16 [2, 31, 1024], P(None, None, 'tp'), may hold values from -1 to 1
- conv_bias: bfloat16 [2, 1024], P(None, 'tp'), may hold values from -3 to 3
- group_gain: bfloat16 [2, 1024], P(None, 'tp'), may hold values from 0.099609375 to 1.8984375
- group_shift: bfloat16 [2, 1024], P(None, 'tp'), may hold values from -3 to 3
- out_proj: bfloat16 [2, 1024, 4096], P(None, 'sp', 'tp'), may hold values from -0.1875 to 0.1875
Outputs:
- hidden_out: bfloat16 [6144, 4096], P('sp', 'tp')
The draws below stay inside these ranges and needn't reach their ends.
All inputs are finite; a program needn't handle non-finite values.
Results may differ from the reference program's by a relative error of at most 0.012.
Values may be sent and summed in bfloat16 or wider, within the bound.
A program may use at most 128 MiB of HBM per device.

```python
import jax
import jax.numpy as jnp
from jax import lax

D = 4096
C = 1024
GROUPS = 4
WIDTH = 31
LAYERS = 2
TOKENS = 6144
N_TP = 4


def draw_hidden_in(key, part):
    first_key, second_key, third_key = jax.random.split(jax.random.fold_in(key, 11), 3)
    phase = jax.random.uniform(first_key, (), jnp.float32)
    columns = jnp.arange(D, dtype=jnp.float32) / D
    column_scale = 0.3 + 1.7 * jnp.mod(columns + phase, 1.0)
    base = jnp.clip(jax.random.normal(second_key, (TOKENS, D), jnp.float32), -6.0, 6.0)
    values = base * column_scale[None, :]
    return values.astype(jnp.bfloat16)


def levels(key, shape, shards, low, high):
    level = 1.0
    for dim, parts in shards:
        steps = jax.random.uniform(jax.random.fold_in(jax.random.fold_in(key, 6), dim), (parts,), jnp.float32, low / len(shards), high / len(shards))
        level = level * jnp.repeat(jnp.exp(steps), shape[dim] // parts).reshape((-1,) + (1,) * (len(shape) - 1 - dim))
    return level


def centred(key, shape, deviation, bound, cuts=(), kind=jnp.bfloat16):
    result = deviation * jax.random.normal(key, shape, jnp.float32)
    if cuts:
        result = result * levels(key, shape, cuts, -0.22, 0.18)
    return jnp.clip(result, -bound, bound).astype(kind)


def setup_inputs(seed: int = 0) -> dict:
    arg_keys = jax.random.split(jax.random.key(seed), 10)
    return {
        "hidden_in": draw_hidden_in(jax.random.fold_in(arg_keys[9], 71), 0),
        "norm_gain": jnp.clip(1.0 + 0.18 * jax.random.normal(arg_keys[1], (LAYERS, D), jnp.float32), 0.099609375, 1.8984375).astype(jnp.bfloat16),
        "value_proj": centred(arg_keys[2], (LAYERS, D, C), D ** -0.5, 0.09375, ((1, 4), (2, 8))),
        "gate_proj": centred(arg_keys[3], (LAYERS, D, C), D ** -0.5, 0.09375, ((1, 4), (2, 8))),
        "conv_taps": centred(arg_keys[4], (LAYERS, WIDTH, C), WIDTH ** -0.5, 1.0, ((2, 4),)),
        "conv_bias": centred(arg_keys[5], (LAYERS, C), 0.5, 3.0, ((1, 4),)),
        "group_gain": jnp.clip(1.0 + 0.18 * jax.random.normal(arg_keys[6], (LAYERS, C), jnp.float32), 0.099609375, 1.8984375).astype(jnp.bfloat16),
        "group_shift": centred(arg_keys[7], (LAYERS, C), 0.5, 3.0, ((1, 4),)),
        "out_proj": centred(arg_keys[8], (LAYERS, C, D), C ** -0.5, 0.1875, ((1, 8), (2, 4))),
    }


row_floor = 1e-06
group_floor = 1e-05

def reference(hidden_in, norm_gain, value_proj, gate_proj, conv_taps, conv_bias, group_gain, group_shift, out_proj):
    residual_rows = hidden_in
    part_width = D // N_TP
    group_size = C // GROUPS
    reach_back = WIDTH - 1
    for level in range(LAYERS):
        wide_rows = residual_rows.astype(jnp.float32)
        scale_rows = lax.rsqrt(lax.optimization_barrier(jnp.mean(wide_rows * wide_rows, axis=1, keepdims=True)) + row_floor)
        normed_rows = (wide_rows * scale_rows * norm_gain[level].astype(jnp.float32)[None, :]).astype(jnp.bfloat16)
        value_sum = jnp.zeros((TOKENS, C), jnp.float32)
        gate_sum = jnp.zeros((TOKENS, C), jnp.float32)
        for block in range(N_TP):
            left_edge = block * part_width
            piece_rows = normed_rows[:, left_edge:left_edge + part_width]
            part_value = jnp.dot(piece_rows, value_proj[level, left_edge:left_edge + part_width], preferred_element_type=jnp.float32).astype(jnp.bfloat16)
            part_gate = jnp.dot(piece_rows, gate_proj[level, left_edge:left_edge + part_width], preferred_element_type=jnp.float32).astype(jnp.bfloat16)
            part_value, part_gate = lax.optimization_barrier((part_value, part_gate))
            value_sum = value_sum + part_value.astype(jnp.float32)
            gate_sum = gate_sum + part_gate.astype(jnp.float32)
        gated = (value_sum * jax.nn.sigmoid(gate_sum)).astype(jnp.bfloat16)
        padded = jnp.pad(gated.astype(jnp.float32), ((reach_back, 0), (0, 0)))
        taps = conv_taps[level].astype(jnp.float32)
        filtered = jnp.zeros((TOKENS, C), jnp.float32) + conv_bias[level].astype(jnp.float32)[None, :]
        for offset in range(WIDTH):
            filtered = filtered + taps[offset][None, :] * padded[offset:offset + TOKENS]
        grouped = filtered.reshape(TOKENS, GROUPS, group_size)
        group_mean = lax.optimization_barrier(jnp.mean(grouped, axis=2, keepdims=True))
        centered = grouped - group_mean
        group_var = lax.optimization_barrier(jnp.mean(centered * centered, axis=2, keepdims=True))
        scaled = (centered * lax.rsqrt(group_var + group_floor)).reshape(TOKENS, C)
        scaled = scaled * group_gain[level].astype(jnp.float32)[None, :] + group_shift[level].astype(jnp.float32)[None, :]
        mixed = jax.nn.silu(scaled).astype(jnp.bfloat16)
        update = jnp.dot(mixed, out_proj[level], preferred_element_type=jnp.float32)
        residual_rows = (wide_rows + update).astype(jnp.bfloat16)
    return residual_rows
```

```python
import jax
import jax.numpy as jnp
from jax import lax
from jax.experimental import pallas as pl
from jax.experimental.pallas import tpu as pltpu
from jax.sharding import PartitionSpec as P

D = 4096
C = 1024
GROUPS = 4
WIDTH = 31


row_floor = 1e-06
group_floor = 1e-05


def passed_along(value, axis, steps):
    count = lax.axis_size(axis)
    initial, last = (max(0, -steps), min(count, count - steps))
    return lax.ppermute(value, axis, [(source, source + steps) for source in range(initial, last)])


def rms_normed(residual_rows, gain_part):
    wide_rows = residual_rows.astype(jnp.float32)
    squares = lax.psum(jnp.sum(wide_rows * wide_rows, axis=1), "tp")
    scale_rows = lax.rsqrt(squares / D + row_floor)
    return (wide_rows * scale_rows[:, None] * gain_part.astype(jnp.float32)[None, :]).astype(
        jnp.bfloat16
    )


def gated_input(normed_rows, w_value, w_gate):
    numbers = (((0,), (1,)), ((), ()))
    value_part = lax.dot_general(w_value, normed_rows, numbers, preferred_element_type=jnp.float32)
    gate_part = lax.dot_general(w_gate, normed_rows, numbers, preferred_element_type=jnp.float32)
    summed = lax.psum_scatter(
        jnp.stack([value_part, gate_part], axis=1).astype(jnp.bfloat16),
        "tp",
        scatter_dimension=0,
        tiled=True,
    ).astype(jnp.float32)
    return (summed[:, 0] * jax.nn.sigmoid(summed[:, 1])).astype(jnp.bfloat16)


def depthwise(extended, taps_part, bias_part, out_len):
    widened = extended.astype(jnp.float32)
    taps = taps_part.astype(jnp.float32)
    filtered = (
        jnp.zeros((extended.shape[0], out_len), jnp.float32)
        + bias_part.astype(jnp.float32)[:, None]
    )
    for offset in range(WIDTH):
        filtered = filtered + taps[offset][:, None] * widened[:, offset : offset + out_len]
    return filtered


def group_normed(filtered, gain_part, shift_part, group_size):
    channels, out_len = filtered.shape
    grouped = filtered.reshape(channels // group_size, group_size, out_len)
    group_mean = jnp.mean(grouped, axis=1, keepdims=True)
    centered = grouped - group_mean
    group_var = jnp.mean(centered * centered, axis=1, keepdims=True)
    scaled = (centered * lax.rsqrt(group_var + group_floor)).reshape(channels, out_len)
    scaled = (
        scaled * gain_part.astype(jnp.float32)[:, None] + shift_part.astype(jnp.float32)[:, None]
    )
    return jax.nn.silu(scaled).astype(jnp.bfloat16)


def project_out(mixed, w_out):
    return lax.dot_general(
        lax.all_gather(mixed, "tp", axis=0, tiled=True),
        w_out,
        (((0,), (0,)), ((), ())),
        preferred_element_type=jnp.float32,
    )


def on_device(
    hidden_in,
    norm_gain,
    value_proj,
    gate_proj,
    conv_taps,
    conv_bias,
    group_gain,
    group_shift,
    out_proj,
):
    tok_rows = hidden_in.shape[0]
    layers = norm_gain.shape[0]
    reach_back = WIDTH - 1
    group_size = C // GROUPS
    all_value, all_gate, all_out = (
        lax.all_gather(value_proj, "sp", axis=2, tiled=True),
        lax.all_gather(gate_proj, "sp", axis=2, tiled=True),
        lax.all_gather(out_proj, "sp", axis=1, tiled=True),
    )
    residual_rows = hidden_in
    for level in range(layers):
        w_value, w_gate, w_out = (all_value[level], all_gate[level], all_out[level])
        normed_rows = rms_normed(residual_rows, norm_gain[level])
        gated = gated_input(normed_rows, w_value, w_gate)
        before = passed_along(gated[:, tok_rows - reach_back :], "sp", 1)
        extended = jnp.concatenate([before, gated], axis=1)
        out_len = extended.shape[1] - reach_back
        filtered = depthwise(extended, conv_taps[level], conv_bias[level], out_len)
        mixed = group_normed(filtered, group_gain[level], group_shift[level], group_size)
        update = project_out(mixed, w_out)
        kept_rows = residual_rows
        residual_rows = (kept_rows.astype(jnp.float32) + update).astype(jnp.bfloat16)
    return residual_rows


MESH = pl.DeviceIdType.MESH
HALO = 32
ROW_TILE = 256
CONV_TILE = 64
VMEM_BYTES = 62 * 1024 * 1024


def fused_kernel(
    n_sp,
    n_tp,
    hidden_ref,
    norm_ref,
    value_ref,
    gate_ref,
    taps_ref,
    bias_ref,
    ggain_ref,
    gshift_ref,
    out_proj_ref,
    out_ref,
    w_in,
    w_out,
    scaled,
    part,
    from_core,
    to_chip,
    from_chip,
    taps,
    extended,
    halo_send,
    halo_recv,
    filtered,
    mixed,
    squares,
    scales,
    load_sem,
    w_send,
    w_recv,
    t_send,
    t_recv,
    s_send,
    s_recv,
):
    width, layers = taps_ref.shape[0], taps_ref.shape[1]
    rows, feats = hidden_ref.shape
    piece = value_ref.shape[2]
    blocks = n_sp // n_tp
    channels = blocks * piece
    reach = width - 1
    nz = n_sp // 2
    s = lax.axis_index("sp")
    t = lax.axis_index("tp")
    z, y = s // 2, s % 2
    chip, core = t // 2, t % 2
    core_mate = chip * 2 + (1 - core)
    chip_mate = (1 - chip) * 2 + core
    far_mate = (1 - chip) * 2 + (1 - core)
    across = z * 2 + 1 - y

    loads = []
    for level in range(layers):
        for kind, (source, target) in enumerate(
            (
                (value_ref.at[level], w_in.at[level, s, :, pl.ds(0, piece)]),
                (gate_ref.at[level], w_in.at[level, s, :, pl.ds(piece, piece)]),
                (
                    out_proj_ref.at[level],
                    w_out.at[level, pl.ds(pl.multiple_of(s * piece, piece), piece), :],
                ),
            )
        ):
            copy = pltpu.make_async_copy(source, target, load_sem.at[level, kind])
            copy.start()
            loads.append(copy)

    barrier = pltpu.get_barrier_semaphore()

    def greet(sp_index, tp_index):
        pl.semaphore_signal(barrier, inc=1, device_id=(sp_index, tp_index), device_id_type=MESH)

    up, down = z < nz - 1, z > 0
    corner_up = jnp.logical_and(up, y == 1)
    corner_down = jnp.logical_and(down, y == 0)
    for mate in (core_mate, chip_mate, far_mate):
        greet(s, mate)
    greet(across, t)
    for condition, target in (
        (up, s + 2),
        (down, s - 2),
        (corner_up, s + 1),
        (corner_down, s - 1),
    ):

        @pl.when(condition)
        def _(target=target):
            greet(target, t)

    mates = 4
    for condition in (up, down, corner_up, corner_down):
        mates = mates + condition.astype(jnp.int32)
    pl.semaphore_wait(barrier, mates)

    for copy in loads:
        copy.wait()

    phases = []
    for level in range(layers):
        phases += [("in", level), ("out", level)]

    def chunk(phase, owner, lot):
        kind, level = phases[phase]
        if kind == "in":
            size = feats // 2
            return w_in.at[level, owner, pl.ds(lot * size, size), :]
        size = piece // 2
        return w_out.at[
            level, pl.ds(pl.multiple_of(owner * piece + lot * size, size), size), :
        ]

    def weight_copy(phase, owner, way, lot):
        return pltpu.make_async_remote_copy(
            src_ref=chunk(phase, owner, lot),
            dst_ref=chunk(phase, owner, lot),
            send_sem=w_send.at[phase, lot, way, owner],
            recv_sem=w_recv.at[phase, lot, owner],
            device_id=((s + 2, s - 2, across)[way], t),
            device_id_type=MESH,
        )

    def go(phase, owner, way, lot, finish):
        copy = weight_copy(phase, owner, way, lot)
        if finish:
            copy.wait_send()
        else:
            copy.start()

    def come(phase, owner, lot, finish):
        if not finish:
            weight_copy(phase, owner, 2, lot).wait_recv()

    def own(phase, finish=False):
        for lot in (1, 0):
            go(phase, s, 2, lot, finish)
        for lot in (0, 1):
            for way, condition in enumerate((up, down)):

                @pl.when(condition)
                def _(way=way, lot=lot):
                    go(phase, s, way, lot, finish)

    def turn(phase, finish=False):
        for way, place in enumerate((0, nz - 1)):

            @pl.when(z == place)
            def _(way=way):
                come(phase, across, 1, finish)
                go(phase, across, way, 1, finish)

    def hop(phase, steps, finish=False):
        for lot in (0, 1):
            for way, sign in enumerate((-1, 1)):
                source = z + sign * steps
                inside = source >= 0 if way == 0 else source < nz
                inner = source > 0 if way == 0 else source < nz - 1
                onward = up if way == 0 else down

                @pl.when(inside)
                def _(way=way, lot=lot, source=source, inner=inner, onward=onward):
                    owner = source * 2 + y
                    come(phase, owner, lot, finish)

                    @pl.when(onward)
                    def _():
                        go(phase, owner, way, lot, finish)

                    if lot == 0:
                        go(phase, owner, 2, lot, finish)
                    else:

                        @pl.when(inner)
                        def _():
                            go(phase, owner, 2, lot, finish)

        for way, place in enumerate((0, nz - 1)):
            source = z - steps if way == 0 else z + steps
            onward = up if way == 0 else down

            @pl.when(source == place)
            def _(way=way, place=place, onward=onward):
                owner = place * 2 + 1 - y
                come(phase, owner, 1, finish)

                @pl.when(onward)
                def _():
                    go(phase, owner, way, 1, finish)

    def crossed(phase, source):
        owner = source * 2 + 1 - y
        come(phase, owner, 0, False)

        @pl.when(jnp.logical_and(source > 0, source < nz - 1))
        def _():
            come(phase, owner, 1, False)

    def sent(phase):
        own(phase, True)
        turn(phase, True)
        for steps in range(1, nz):
            hop(phase, steps, True)

    def tp_copy(level, slot, source, target, mate, sp_index=None):
        return pltpu.make_async_remote_copy(
            src_ref=source,
            dst_ref=target,
            send_sem=t_send.at[level, slot],
            recv_sem=t_recv.at[level, slot],
            device_id=(s if sp_index is None else sp_index, mate),
            device_id_type=MESH,
        )

    tiles = rows // ROW_TILE
    order = tuple(reversed(range(tiles)))

    def prepare(level, tile):
        gain = norm_ref[pl.ds(level, 1), :].astype(jnp.float32)
        ones = jnp.ones((8, feats), jnp.bfloat16)
        numbers = (((1,), (1,)), ((), ()))
        source = hidden_ref if level == 0 else out_ref
        span = pl.ds(tile * ROW_TILE, ROW_TILE)
        wide = source[span, :].astype(jnp.float32)
        scaled[span, :] = (wide * gain).astype(jnp.bfloat16)
        square = wide * wide
        high = square.astype(jnp.bfloat16)
        low = (square - high.astype(jnp.float32)).astype(jnp.bfloat16)
        total = lax.dot_general(ones, high, numbers, preferred_element_type=jnp.float32)
        total = total + lax.dot_general(ones, low, numbers, preferred_element_type=jnp.float32)
        squares[level, t, :, span] = total

    def square_copies(level):
        return [
            pltpu.make_async_remote_copy(
                src_ref=squares.at[level, t],
                dst_ref=squares.at[level, t],
                send_sem=s_send.at[level, slot],
                recv_sem=s_recv.at[level, slot],
                device_id=(s, mate),
                device_id_type=MESH,
            )
            for slot, mate in enumerate((core_mate, chip_mate, far_mate))
        ]

    def row_scales(level):
        for copy in square_copies(level):
            copy.wait_send()
            copy.wait_recv()
        total = squares[level, 0]
        for index in range(1, n_tp):
            total = total + squares[level, index]
        scales[...] = lax.rsqrt(total / D + row_floor).T

    def core_copy(level, target_chip, block):
        owner = target_chip * 2 + 1 - core
        return tp_copy(
            level,
            target_chip * blocks + block,
            part.at[owner, block],
            from_core.at[level, target_chip, block],
            core_mate,
        )

    base = 2 * blocks

    def chip_copy(level, block):
        return tp_copy(
            level, base + block, to_chip.at[block], from_chip.at[level, block], chip_mate
        )

    def halo_copy(level, block):
        return tp_copy(
            level,
            base + blocks + block,
            halo_send.at[block],
            halo_recv.at[level, block],
            t,
            s + 1,
        )

    def mixed_copy(level, slot, third):
        owner = (t, t, chip_mate)[slot]
        mate = (core_mate, chip_mate, core_mate)[slot]
        block = mixed.at[level, owner, pl.ds(third * ROW_TILE, ROW_TILE), :]
        return tp_copy(level, base + 2 * blocks + slot * tiles + third, block, block, mate)

    def target_of(turn_index):
        upper = z // (nz // 2)
        near = z + upper * (nz - 1 - 2 * z)
        pick = (near, 1 - near)[turn_index] if turn_index < 2 else turn_index
        return pick + upper * (nz - 1 - 2 * pick)

    def products(level, target, block):
        @pl.loop(0, tiles)
        def _(tile):
            span = pl.ds(pl.multiple_of(tile * ROW_TILE, ROW_TILE), ROW_TILE)
            part[target, block, span, :] = jnp.dot(
                scaled[span, :],
                w_in[level, target * blocks + block],
                preferred_element_type=jnp.float32,
            ).astype(jnp.bfloat16)

        @pl.when(target % 2 != core)
        def _():
            core_copy(level, target // 2, block).start()

    def contribute(level, target):
        products(level, target, y)
        crossed(2 * level, target)
        products(level, target, 1 - y)

    def pass_on(level, target):
        @pl.when(target == chip_mate)
        def _():
            for turn_index in range(blocks):
                block = (y + turn_index) % blocks
                core_copy(level, 1 - chip, block).wait_recv()

                @pl.loop(0, tiles)
                def _(tile, block=block):
                    span = pl.ds(pl.multiple_of(tile * ROW_TILE, ROW_TILE), ROW_TILE)
                    to_chip[block, span, :] = (
                        part[chip_mate, block, span, :].astype(jnp.float32)
                        + from_core[level, 1 - chip, block, span, :].astype(jnp.float32)
                    ).astype(jnp.bfloat16)

                chip_copy(level, block).start()

    def gating(level, block):
        core_copy(level, chip, block).wait_recv()
        chip_copy(level, block).wait_recv()

        @pl.loop(0, tiles)
        def _(tile):
            start = pl.multiple_of(tile * ROW_TILE, ROW_TILE)
            span = pl.ds(start, ROW_TILE)
            total = (
                part[t, block, span, :].astype(jnp.float32)
                + from_core[level, chip, block, span, :].astype(jnp.float32)
                + from_chip[level, block, span, :].astype(jnp.float32)
            ) * scales[span, 0:1]
            gated = (total[:, :piece] * jax.nn.sigmoid(total[:, piece:])).astype(jnp.bfloat16)
            extended[block, pl.ds(HALO + start, ROW_TILE), :] = gated.astype(jnp.float32)

        halo_send[block] = extended[block, pl.ds(rows, HALO), :].astype(jnp.bfloat16)

        @pl.when(s < n_sp - 1)
        def _():
            halo_copy(level, block).start()

    per_part = ROW_TILE // CONV_TILE

    def convolve(level, block, third):
        bias = taps[level, block, pl.ds(width, 1), :]
        weights = taps[level, block]

        @pl.loop(third * per_part, (third + 1) * per_part)
        def _(tile):
            start = pl.multiple_of(tile * CONV_TILE, CONV_TILE)
            window = extended[block, pl.ds(start, CONV_TILE + HALO), :]
            total = jnp.zeros((CONV_TILE, piece), jnp.float32) + bias
            for offset in range(width):
                low = HALO - reach + offset
                total = total + weights[offset : offset + 1, :] * window[low : low + CONV_TILE]
            filtered[block, pl.ds(start, CONV_TILE), :] = total

    def first_rows(level, block):
        @pl.when(s > 0)
        def _():
            halo_copy(level, block).wait_recv()
            extended[block, pl.ds(0, HALO), :] = halo_recv[level, block].astype(jnp.float32)

        @pl.when(s == 0)
        def _():
            extended[block, pl.ds(0, HALO), :] = jnp.zeros((HALO, piece), jnp.float32)

    def normalise(level, third):
        ggain = ggain_ref[pl.ds(level, 1), :].astype(jnp.float32)
        gshift = gshift_ref[pl.ds(level, 1), :].astype(jnp.float32)

        @pl.loop(third * per_part, (third + 1) * per_part)
        def _(tile):
            span = pl.ds(pl.multiple_of(tile * CONV_TILE, CONV_TILE), CONV_TILE)
            pieces = [filtered[block, span, :] for block in range(blocks)]
            mean = sum(jnp.sum(value, axis=1, keepdims=True) for value in pieces) / channels
            pieces = [value - mean for value in pieces]
            var = sum(jnp.sum(value * value, axis=1, keepdims=True) for value in pieces) / channels
            factor = lax.rsqrt(var + group_floor)
            for block in range(blocks):
                lanes = slice(block * piece, (block + 1) * piece)
                normed = pieces[block] * factor * ggain[:, lanes] + gshift[:, lanes]
                mixed[level, t, span, lanes] = (normed * jax.nn.sigmoid(normed)).astype(
                    jnp.bfloat16
                )

        mixed_copy(level, 1, third).start()
        mixed_copy(level, 0, third).start()

    def relay(level, third):
        mixed_copy(level, 1, third).wait_recv()
        mixed_copy(level, 2, third).start()

    def projecting(level, third):
        mixed_copy(level, 0, third).wait_recv()
        mixed_copy(level, 2, third).wait_recv()
        source = hidden_ref if level == 0 else out_ref
        span = pl.ds(third * ROW_TILE, ROW_TILE)
        total = source[span, :].astype(jnp.float32)
        for owner in range(n_tp):
            total = total + jnp.dot(
                mixed[level, owner, span, :],
                w_out[level, pl.ds(owner * channels, channels), :],
                preferred_element_type=jnp.float32,
            )
        out_ref[span, :] = total.astype(jnp.bfloat16)
        if level + 1 < layers:
            prepare(level + 1, third)

    def settle(level):
        for target_chip in range(2):
            for block in range(blocks):
                core_copy(level, target_chip, block).wait_send()
        for block in range(blocks):
            chip_copy(level, block).wait_send()
        for slot in range(3):
            for third in order:
                mixed_copy(level, slot, third).wait_send()

        @pl.when(s < n_sp - 1)
        def _():
            for block in range(blocks):
                halo_copy(level, block).wait_send()

    own(0)
    for level in range(layers):
        for block in range(blocks):
            lanes = slice(block * piece, (block + 1) * piece)
            taps[level, block, 0:width, :] = taps_ref[:, level, lanes].astype(jnp.float32)
            taps[level, block, width : width + 1, :] = bias_ref[level : level + 1, lanes].astype(
                jnp.float32
            )
    for tile in range(tiles):
        prepare(0, tile)
    for copy in square_copies(0):
        copy.start()
    turn(0)
    for level in range(layers):
        first, second = 2 * level, 2 * level + 1
        last = level == layers - 1
        targets = [target_of(turn_index) for turn_index in range(n_tp)]
        hop(first, 1)
        contribute(level, targets[0])
        hop(first, 2)
        own(second)
        pass_on(level, targets[0])
        contribute(level, targets[1])
        turn(second)
        pass_on(level, targets[1])
        hop(first, 3)
        contribute(level, targets[2])
        pass_on(level, targets[2])
        contribute(level, targets[3])
        pass_on(level, targets[3])
        hop(second, 1)
        row_scales(level)
        gating(level, y)
        for third in order[:-1]:
            convolve(level, y, third)
        hop(second, 2)
        if not last:
            own(first + 2)
        gating(level, 1 - y)
        for third in order[:-1]:
            convolve(level, 1 - y, third)
            normalise(level, third)
        if not last:
            turn(first + 2)
        for block in (y, 1 - y):
            first_rows(level, block)
            convolve(level, block, order[-1])
        normalise(level, order[-1])
        hop(second, 3)
        relay(level, order[0])
        for source in range(nz):
            crossed(second, source)
        for index in range(1, tiles):
            relay(level, order[index])
            projecting(level, order[index - 1])
        projecting(level, order[-1])
        if not last:
            for copy in square_copies(level + 1):
                copy.start()
        settle(level)
    for phase in range(len(phases)):
        sent(phase)


def fused(n_sp, n_tp, *arrays):
    hidden_in, norm_gain, value_proj = arrays[:3]
    rows, feats = hidden_in.shape
    layers = norm_gain.shape[0]
    piece = value_proj.shape[2]
    blocks = n_sp // n_tp
    channels = blocks * piece
    kinds = 3
    vmem = pl.BlockSpec(memory_space=pltpu.VMEM)
    hbm = pl.BlockSpec(memory_space=pl.ANY)
    low, wide = jnp.bfloat16, jnp.float32
    slots = 4 * blocks + 3 * (rows // ROW_TILE)
    arrays = arrays[:4] + (arrays[4].transpose(1, 0, 2),) + arrays[5:]
    return pl.pallas_call(
        lambda *refs: fused_kernel(n_sp, n_tp, *refs),
        out_shape=jax.ShapeDtypeStruct((rows, feats), low),
        in_specs=[vmem, vmem, hbm, hbm, vmem, vmem, vmem, vmem, hbm],
        out_specs=vmem,
        scratch_shapes=[
            pltpu.VMEM((layers, n_sp, feats, 2 * piece), low),
            pltpu.VMEM((layers, n_sp * piece, feats), low),
            pltpu.VMEM((rows, feats), low),
            pltpu.VMEM((n_tp, blocks, rows, 2 * piece), low),
            pltpu.VMEM((layers, 2, blocks, rows, 2 * piece), low),
            pltpu.VMEM((blocks, rows, 2 * piece), low),
            pltpu.VMEM((layers, blocks, rows, 2 * piece), low),
            pltpu.VMEM((layers, blocks, WIDTH + 1, piece), wide),
            pltpu.VMEM((blocks, HALO + rows, piece), wide),
            pltpu.VMEM((blocks, HALO, piece), low),
            pltpu.VMEM((layers, blocks, HALO, piece), low),
            pltpu.VMEM((blocks, rows, piece), wide),
            pltpu.VMEM((layers, n_tp, rows, channels), low),
            pltpu.VMEM((layers, n_tp, 8, rows), wide),
            pltpu.VMEM((rows, 8), wide),
            pltpu.SemaphoreType.DMA((layers, kinds)),
            pltpu.SemaphoreType.DMA((layers * 2, 2, 3, n_sp)),
            pltpu.SemaphoreType.DMA((layers * 2, 2, n_sp)),
            pltpu.SemaphoreType.DMA((layers, slots)),
            pltpu.SemaphoreType.DMA((layers, slots)),
            pltpu.SemaphoreType.DMA((layers, 3)),
            pltpu.SemaphoreType.DMA((layers, 3)),
        ],
        compiler_params=pltpu.CompilerParams(
            collective_id=0, has_side_effects=True, vmem_limit_bytes=VMEM_BYTES
        ),
    )(*arrays)


def solution(mesh):
    n_sp, n_tp = mesh.shape["sp"], mesh.shape["tp"]
    piece = C // n_sp
    small = n_tp == 4 and GROUPS == n_tp and n_sp == 2 * n_tp and piece % 128 == 0

    def local(*arrays):
        if small and arrays[0].shape[0] % ROW_TILE == 0:
            return fused(n_sp, n_tp, *arrays)
        return on_device(*arrays)

    return jax.shard_map(
        local,
        mesh=mesh,
        in_specs=(
            P("sp", "tp"),
            P(None, "tp"),
            P(None, "tp", "sp"),
            P(None, "tp", "sp"),
            P(None, None, "tp"),
            P(None, "tp"),
            P(None, "tp"),
            P(None, "tp"),
            P(None, "sp", "tp"),
        ),
        out_specs=P("sp", "tp"),
        check_vma=False,
    )
```

```python
import jax
import jax.numpy as jnp
from jax import lax
from jax.experimental import pallas as pl
from jax.experimental.pallas import tpu as pltpu
from jax.sharding import PartitionSpec as P

D = 4096
C = 1024
GROUPS = 4
WIDTH = 31


row_floor = 1e-06
group_floor = 1e-05


def passed_along(value, axis, steps):
    count = lax.axis_size(axis)
    initial, last = (max(0, -steps), min(count, count - steps))
    return lax.ppermute(value, axis, [(source, source + steps) for source in range(initial, last)])


def rms_normed(residual_rows, gain_part):
    wide_rows = residual_rows.astype(jnp.float32)
    squares = lax.psum(jnp.sum(wide_rows * wide_rows, axis=1), "tp")
    scale_rows = lax.rsqrt(squares / D + row_floor)
    return (wide_rows * scale_rows[:, None] * gain_part.astype(jnp.float32)[None, :]).astype(
        jnp.bfloat16
    )


def gated_input(normed_rows, w_value, w_gate):
    numbers = (((0,), (1,)), ((), ()))
    value_part = lax.dot_general(w_value, normed_rows, numbers, preferred_element_type=jnp.float32)
    gate_part = lax.dot_general(w_gate, normed_rows, numbers, preferred_element_type=jnp.float32)
    summed = lax.psum_scatter(
        jnp.stack([value_part, gate_part], axis=1).astype(jnp.bfloat16),
        "tp",
        scatter_dimension=0,
        tiled=True,
    ).astype(jnp.float32)
    return (summed[:, 0] * jax.nn.sigmoid(summed[:, 1])).astype(jnp.bfloat16)


def depthwise(extended, taps_part, bias_part, out_len):
    widened = extended.astype(jnp.float32)
    taps = taps_part.astype(jnp.float32)
    filtered = (
        jnp.zeros((extended.shape[0], out_len), jnp.float32)
        + bias_part.astype(jnp.float32)[:, None]
    )
    for offset in range(WIDTH):
        filtered = filtered + taps[offset][:, None] * widened[:, offset : offset + out_len]
    return filtered


def group_normed(filtered, gain_part, shift_part, group_size):
    channels, out_len = filtered.shape
    grouped = filtered.reshape(channels // group_size, group_size, out_len)
    group_mean = jnp.mean(grouped, axis=1, keepdims=True)
    centered = grouped - group_mean
    group_var = jnp.mean(centered * centered, axis=1, keepdims=True)
    scaled = (centered * lax.rsqrt(group_var + group_floor)).reshape(channels, out_len)
    scaled = (
        scaled * gain_part.astype(jnp.float32)[:, None] + shift_part.astype(jnp.float32)[:, None]
    )
    return jax.nn.silu(scaled).astype(jnp.bfloat16)


def project_out(mixed, w_out):
    return lax.dot_general(
        lax.all_gather(mixed, "tp", axis=0, tiled=True),
        w_out,
        (((0,), (0,)), ((), ())),
        preferred_element_type=jnp.float32,
    )


def on_device(
    hidden_in,
    norm_gain,
    value_proj,
    gate_proj,
    conv_taps,
    conv_bias,
    group_gain,
    group_shift,
    out_proj,
):
    tok_rows = hidden_in.shape[0]
    layers = norm_gain.shape[0]
    reach_back = WIDTH - 1
    group_size = C // GROUPS
    all_value, all_gate, all_out = (
        lax.all_gather(value_proj, "sp", axis=2, tiled=True),
        lax.all_gather(gate_proj, "sp", axis=2, tiled=True),
        lax.all_gather(out_proj, "sp", axis=1, tiled=True),
    )
    residual_rows = hidden_in
    for level in range(layers):
        w_value, w_gate, w_out = (all_value[level], all_gate[level], all_out[level])
        normed_rows = rms_normed(residual_rows, norm_gain[level])
        gated = gated_input(normed_rows, w_value, w_gate)
        before = passed_along(gated[:, tok_rows - reach_back :], "sp", 1)
        extended = jnp.concatenate([before, gated], axis=1)
        out_len = extended.shape[1] - reach_back
        filtered = depthwise(extended, conv_taps[level], conv_bias[level], out_len)
        mixed = group_normed(filtered, group_gain[level], group_shift[level], group_size)
        update = project_out(mixed, w_out)
        kept_rows = residual_rows
        residual_rows = (kept_rows.astype(jnp.float32) + update).astype(jnp.bfloat16)
    return residual_rows


MESH = pl.DeviceIdType.MESH
HALO = 32
ROW_TILE = 256
CONV_TILE = 64
VMEM_BYTES = 62 * 1024 * 1024


def fused_kernel(
    n_sp,
    n_tp,
    hidden_ref,
    norm_ref,
    value_ref,
    gate_ref,
    taps_ref,
    bias_ref,
    ggain_ref,
    gshift_ref,
    out_proj_ref,
    out_ref,
    w_in,
    w_out,
    scaled,
    part,
    from_core,
    to_chip,
    from_chip,
    taps,
    extended,
    halo_send,
    halo_recv,
    filtered,
    mixed,
    squares,
    scales,
    load_sem,
    w_send,
    w_recv,
    t_send,
    t_recv,
    s_send,
    s_recv,
):
    width, layers = taps_ref.shape[0], taps_ref.shape[1]
    rows, feats = hidden_ref.shape
    piece = value_ref.shape[2]
    blocks = n_sp // n_tp
    channels = blocks * piece
    reach = width - 1
    nz = n_sp // 2
    s = lax.axis_index("sp")
    t = lax.axis_index("tp")
    z, y = s // 2, s % 2
    chip, core = t // 2, t % 2
    core_mate = chip * 2 + (1 - core)
    chip_mate = (1 - chip) * 2 + core
    far_mate = (1 - chip) * 2 + (1 - core)
    across = z * 2 + 1 - y

    loads = []
    for level in range(layers):
        for kind, (source, target) in enumerate(
            (
                (value_ref.at[level], w_in.at[level, s, :, pl.ds(0, piece)]),
                (gate_ref.at[level], w_in.at[level, s, :, pl.ds(piece, piece)]),
                (
                    out_proj_ref.at[level],
                    w_out.at[level, pl.ds(pl.multiple_of(s * piece, piece), piece), :],
                ),
            )
        ):
            copy = pltpu.make_async_copy(source, target, load_sem.at[level, kind])
            copy.start()
            loads.append(copy)

    barrier = pltpu.get_barrier_semaphore()

    def greet(sp_index, tp_index):
        pl.semaphore_signal(barrier, inc=1, device_id=(sp_index, tp_index), device_id_type=MESH)

    up, down = z < nz - 1, z > 0
    corner_up = jnp.logical_and(up, y == 1)
    corner_down = jnp.logical_and(down, y == 0)
    for mate in (core_mate, chip_mate, far_mate):
        greet(s, mate)
    greet(across, t)
    for condition, target in (
        (up, s + 2),
        (down, s - 2),
        (corner_up, s + 1),
        (corner_down, s - 1),
    ):

        @pl.when(condition)
        def _(target=target):
            greet(target, t)

    mates = 4
    for condition in (up, down, corner_up, corner_down):
        mates = mates + condition.astype(jnp.int32)
    pl.semaphore_wait(barrier, mates)

    for copy in loads:
        copy.wait()

    phases = []
    for level in range(layers):
        phases += [("in", level), ("out", level)]

    def chunk(phase, owner, lot):
        kind, level = phases[phase]
        if kind == "in":
            size = feats // 2
            return w_in.at[level, owner, pl.ds(lot * size, size), :]
        size = piece // 2
        return w_out.at[
            level, pl.ds(pl.multiple_of(owner * piece + lot * size, size), size), :
        ]

    def weight_copy(phase, owner, way, lot):
        return pltpu.make_async_remote_copy(
            src_ref=chunk(phase, owner, lot),
            dst_ref=chunk(phase, owner, lot),
            send_sem=w_send.at[phase, lot, way, owner],
            recv_sem=w_recv.at[phase, lot, owner],
            device_id=((s + 2, s - 2, across)[way], t),
            device_id_type=MESH,
        )

    def go(phase, owner, way, lot, finish):
        copy = weight_copy(phase, owner, way, lot)
        if finish:
            copy.wait_send()
        else:
            copy.start()

    def come(phase, owner, lot, finish):
        if not finish:
            weight_copy(phase, owner, 2, lot).wait_recv()

    outer = jnp.logical_or(z == 0, z == nz - 1)
    middle = jnp.logical_and(z > 0, z < nz - 1)

    def own_rows(phase, finish=False):
        for lot in (1, 0):
            go(phase, s, 2, lot, finish)

    def own_column(phase, finish=False):
        for lot in (0, 1):
            for way, condition in enumerate((up, down)):

                @pl.when(condition)
                def _(way=way, lot=lot):
                    go(phase, s, way, lot, finish)

    def turn(phase, finish=False):
        for way, place in enumerate((0, nz - 1)):

            @pl.when(z == place)
            def _(way=way):
                come(phase, across, 1, finish)
                go(phase, across, way, 1, finish)

    def hop(phase, steps, lots=(0, 1), finish=False):
        for lot in lots:
            for way, sign in enumerate((-1, 1)):
                source = z + sign * steps
                inside = source >= 0 if way == 0 else source < nz
                inner = source > 0 if way == 0 else source < nz - 1
                onward = up if way == 0 else down

                @pl.when(inside)
                def _(way=way, lot=lot, source=source, inner=inner, onward=onward):
                    owner = source * 2 + y
                    come(phase, owner, lot, finish)

                    @pl.when(onward)
                    def _():
                        go(phase, owner, way, lot, finish)

                    if lot == 0:
                        go(phase, owner, 2, lot, finish)
                    else:

                        @pl.when(inner)
                        def _():
                            go(phase, owner, 2, lot, finish)

    def side(phase, steps, finish=False):
        for way, place in enumerate((0, nz - 1)):
            source = z - steps if way == 0 else z + steps
            onward = up if way == 0 else down

            @pl.when(source == place)
            def _(way=way, place=place, onward=onward):
                owner = place * 2 + 1 - y
                come(phase, owner, 1, finish)

                @pl.when(onward)
                def _():
                    go(phase, owner, way, 1, finish)

    def apart(condition, *steps):
        @pl.when(condition)
        def _():
            for function, *arguments in steps:
                function(*arguments)

    def crossed(phase, source):
        owner = source * 2 + 1 - y
        come(phase, owner, 0, False)

        @pl.when(jnp.logical_and(source > 0, source < nz - 1))
        def _():
            come(phase, owner, 1, False)

    def sent(phase):
        own_rows(phase, True)
        own_column(phase, True)
        turn(phase, True)
        for steps in range(1, nz):
            hop(phase, steps, finish=True)
            side(phase, steps, True)

    def tp_copy(level, slot, source, target, mate, sp_index=None):
        return pltpu.make_async_remote_copy(
            src_ref=source,
            dst_ref=target,
            send_sem=t_send.at[level, slot],
            recv_sem=t_recv.at[level, slot],
            device_id=(s if sp_index is None else sp_index, mate),
            device_id_type=MESH,
        )

    tiles = rows // ROW_TILE
    order = tuple(reversed(range(tiles)))

    def prepare(level, tile):
        gain = norm_ref[pl.ds(level, 1), :].astype(jnp.float32)
        ones = jnp.ones((8, feats), jnp.bfloat16)
        numbers = (((1,), (1,)), ((), ()))
        source = hidden_ref if level == 0 else out_ref
        span = pl.ds(tile * ROW_TILE, ROW_TILE)
        wide = source[span, :].astype(jnp.float32)
        scaled[span, :] = (wide * gain).astype(jnp.bfloat16)
        square = wide * wide
        high = square.astype(jnp.bfloat16)
        low = (square - high.astype(jnp.float32)).astype(jnp.bfloat16)
        total = lax.dot_general(ones, high, numbers, preferred_element_type=jnp.float32)
        total = total + lax.dot_general(ones, low, numbers, preferred_element_type=jnp.float32)
        squares[level, t, :, span] = total

    def square_copies(level):
        return [
            pltpu.make_async_remote_copy(
                src_ref=squares.at[level, t],
                dst_ref=squares.at[level, t],
                send_sem=s_send.at[level, slot],
                recv_sem=s_recv.at[level, slot],
                device_id=(s, mate),
                device_id_type=MESH,
            )
            for slot, mate in enumerate((core_mate, chip_mate, far_mate))
        ]

    def row_scales(level):
        for copy in square_copies(level):
            copy.wait_send()
            copy.wait_recv()
        total = squares[level, 0]
        for index in range(1, n_tp):
            total = total + squares[level, index]
        scales[...] = lax.rsqrt(total / D + row_floor).T

    def core_copy(level, target_chip, block):
        owner = target_chip * 2 + 1 - core
        return tp_copy(
            level,
            target_chip * blocks + block,
            part.at[owner, block],
            from_core.at[level, target_chip, block],
            core_mate,
        )

    base = 2 * blocks

    def chip_copy(level, block):
        return tp_copy(
            level, base + block, to_chip.at[block], from_chip.at[level, block], chip_mate
        )

    def halo_copy(level, block):
        return tp_copy(
            level,
            base + blocks + block,
            halo_send.at[block],
            halo_recv.at[level, block],
            t,
            s + 1,
        )

    def mixed_copy(level, slot, third):
        owner = (t, t, chip_mate)[slot]
        mate = (core_mate, chip_mate, core_mate)[slot]
        block = mixed.at[level, owner, pl.ds(third * ROW_TILE, ROW_TILE), :]
        return tp_copy(level, base + 2 * blocks + slot * tiles + third, block, block, mate)

    def target_of(turn_index):
        upper = z // (nz // 2)
        near = z + upper * (nz - 1 - 2 * z)
        pick = (near, 1 - near)[turn_index] if turn_index < 2 else turn_index
        return pick + upper * (nz - 1 - 2 * pick)

    def products(level, target, block):
        @pl.loop(0, tiles)
        def _(tile):
            span = pl.ds(pl.multiple_of(tile * ROW_TILE, ROW_TILE), ROW_TILE)
            part[target, block, span, :] = jnp.dot(
                scaled[span, :],
                w_in[level, target * blocks + block],
                preferred_element_type=jnp.float32,
            ).astype(jnp.bfloat16)

        @pl.when(target % 2 != core)
        def _():
            core_copy(level, target // 2, block).start()

    def contribute(level, target, turned):
        block = 1 - y if turned else y
        if turned:
            crossed(2 * level, target)
        products(level, target, block)

    def pass_on(level, target, turned):
        block = 1 - y if turned else y

        @pl.when(target == chip_mate)
        def _():
            core_copy(level, 1 - chip, block).wait_recv()

            @pl.loop(0, tiles)
            def _(tile):
                span = pl.ds(pl.multiple_of(tile * ROW_TILE, ROW_TILE), ROW_TILE)
                to_chip[block, span, :] = (
                    part[chip_mate, block, span, :].astype(jnp.float32)
                    + from_core[level, 1 - chip, block, span, :].astype(jnp.float32)
                ).astype(jnp.bfloat16)

            chip_copy(level, block).start()

    def gating(level, block):
        core_copy(level, chip, block).wait_recv()
        chip_copy(level, block).wait_recv()

        @pl.loop(0, tiles)
        def _(tile):
            start = pl.multiple_of(tile * ROW_TILE, ROW_TILE)
            span = pl.ds(start, ROW_TILE)
            total = (
                part[t, block, span, :].astype(jnp.float32)
                + from_core[level, chip, block, span, :].astype(jnp.float32)
                + from_chip[level, block, span, :].astype(jnp.float32)
            ) * scales[span, 0:1]
            gated = (total[:, :piece] * jax.nn.sigmoid(total[:, piece:])).astype(jnp.bfloat16)
            extended[block, pl.ds(HALO + start, ROW_TILE), :] = gated.astype(jnp.float32)

        halo_send[block] = extended[block, pl.ds(rows, HALO), :].astype(jnp.bfloat16)

        @pl.when(s < n_sp - 1)
        def _():
            halo_copy(level, block).start()

    per_part = ROW_TILE // CONV_TILE

    def convolve(level, block, third):
        bias = taps[level, block, pl.ds(width, 1), :]
        weights = taps[level, block]

        @pl.loop(third * per_part, (third + 1) * per_part)
        def _(tile):
            start = pl.multiple_of(tile * CONV_TILE, CONV_TILE)
            window = extended[block, pl.ds(start, CONV_TILE + HALO), :]
            total = jnp.zeros((CONV_TILE, piece), jnp.float32) + bias
            for offset in range(width):
                low = HALO - reach + offset
                total = total + weights[offset : offset + 1, :] * window[low : low + CONV_TILE]
            filtered[block, pl.ds(start, CONV_TILE), :] = total

    def first_rows(level, block):
        @pl.when(s > 0)
        def _():
            halo_copy(level, block).wait_recv()
            extended[block, pl.ds(0, HALO), :] = halo_recv[level, block].astype(jnp.float32)

        @pl.when(s == 0)
        def _():
            extended[block, pl.ds(0, HALO), :] = jnp.zeros((HALO, piece), jnp.float32)

    def normalise(level, third):
        ggain = ggain_ref[pl.ds(level, 1), :].astype(jnp.float32)
        gshift = gshift_ref[pl.ds(level, 1), :].astype(jnp.float32)

        @pl.loop(third * per_part, (third + 1) * per_part)
        def _(tile):
            span = pl.ds(pl.multiple_of(tile * CONV_TILE, CONV_TILE), CONV_TILE)
            pieces = [filtered[block, span, :] for block in range(blocks)]
            mean = sum(jnp.sum(value, axis=1, keepdims=True) for value in pieces) / channels
            pieces = [value - mean for value in pieces]
            var = sum(jnp.sum(value * value, axis=1, keepdims=True) for value in pieces) / channels
            factor = lax.rsqrt(var + group_floor)
            for block in range(blocks):
                lanes = slice(block * piece, (block + 1) * piece)
                normed = pieces[block] * factor * ggain[:, lanes] + gshift[:, lanes]
                mixed[level, t, span, lanes] = (normed * jax.nn.sigmoid(normed)).astype(
                    jnp.bfloat16
                )

        mixed_copy(level, 1, third).start()
        mixed_copy(level, 0, third).start()

    def relay(level, third):
        mixed_copy(level, 1, third).wait_recv()
        mixed_copy(level, 2, third).start()

    def projecting(level, third):
        mixed_copy(level, 0, third).wait_recv()
        mixed_copy(level, 2, third).wait_recv()
        source = hidden_ref if level == 0 else out_ref
        span = pl.ds(third * ROW_TILE, ROW_TILE)
        total = source[span, :].astype(jnp.float32)
        for owner in range(n_tp):
            total = total + jnp.dot(
                mixed[level, owner, span, :],
                w_out[level, pl.ds(owner * channels, channels), :],
                preferred_element_type=jnp.float32,
            )
        out_ref[span, :] = total.astype(jnp.bfloat16)
        if level + 1 < layers:
            prepare(level + 1, third)

    def settle(level):
        for target_chip in range(2):
            for block in range(blocks):
                core_copy(level, target_chip, block).wait_send()
        for block in range(blocks):
            chip_copy(level, block).wait_send()
        for slot in range(3):
            for third in order:
                mixed_copy(level, slot, third).wait_send()

        @pl.when(s < n_sp - 1)
        def _():
            for block in range(blocks):
                halo_copy(level, block).wait_send()

    own_rows(0)
    own_column(0)
    for level in range(layers):
        for block in range(blocks):
            lanes = slice(block * piece, (block + 1) * piece)
            taps[level, block, 0:width, :] = taps_ref[:, level, lanes].astype(jnp.float32)
            taps[level, block, width : width + 1, :] = bias_ref[level : level + 1, lanes].astype(
                jnp.float32
            )
    for tile in range(tiles):
        prepare(0, tile)
    for copy in square_copies(0):
        copy.start()
    apart(outer, (turn, 0), *((own_column, phase) for phase in range(1, len(phases))))
    end = outer.astype(jnp.int32)
    for level in range(layers):
        first, second = 2 * level, 2 * level + 1
        last = level == layers - 1
        targets = [target_of(turn_index) for turn_index in range(n_tp)]
        third_target = targets[2] * end + targets[3] * (1 - end)
        contribute(level, targets[0], 0)
        if level == 0:
            hop(first, 1)
        else:
            apart(outer, (turn, first), (hop, first, 1, (1,)))
        contribute(level, targets[1], 0)
        apart(middle, (contribute, level, targets[2], 0))
        contribute(level, targets[0], 1)
        pass_on(level, targets[0], 0)
        apart(middle, (side, first, 1))
        if level == 0:
            hop(first, 2)
        else:
            apart(outer, (hop, first, 2))
        pass_on(level, targets[1], 0)
        apart(middle, (pass_on, level, targets[2], 0))
        contribute(level, third_target, 0)
        pass_on(level, targets[0], 1)
        contribute(level, targets[1], 1)
        apart(
            outer,
            (hop, first, 3),
            (own_rows, second),
            (contribute, level, targets[3], 0),
        )
        pass_on(level, third_target, 0)
        pass_on(level, targets[1], 1)
        contribute(level, targets[2], 1)
        apart(outer, (pass_on, level, targets[3], 0))
        pass_on(level, targets[2], 1)
        apart(outer, (side, first, nz - 1))
        apart(middle, (side, first, nz - 2), (own_rows, second), (own_column, second))
        contribute(level, targets[3], 1)
        pass_on(level, targets[3], 1)
        apart(outer, (turn, second), (hop, second, 1), (hop, second, 2, (0,)))
        apart(middle, (hop, second, 1))
        row_scales(level)
        gating(level, y)
        for third in order[:-1]:
            convolve(level, y, third)
        apart(outer, (hop, second, 2, (1,)))
        gating(level, 1 - y)
        apart(middle, (hop, second, 2))
        for third in order[:-1]:
            convolve(level, 1 - y, third)
            normalise(level, third)
            if third == order[0]:
                apart(outer, (hop, second, 3, (0,)))
                if not last:
                    apart(outer, (own_rows, first + 2))
        apart(middle, (side, second, 1), (side, second, 2))
        if not last:
            apart(middle, (own_rows, first + 2), (own_column, first + 2))
        for block in (y, 1 - y):
            first_rows(level, block)
            convolve(level, block, order[-1])
        normalise(level, order[-1])
        relay(level, order[0])
        apart(outer, (hop, second, 3, (1,)), (side, second, nz - 1))
        for source in range(nz):
            crossed(second, source)
        for index in range(1, tiles):
            relay(level, order[index])
            projecting(level, order[index - 1])
        if not last:
            apart(middle, (hop, first + 2, 1))
            apart(outer, (hop, first + 2, 1, (0,)))
        projecting(level, order[-1])
        if not last:
            for copy in square_copies(level + 1):
                copy.start()
            apart(middle, (hop, first + 2, 2))
        settle(level)
    for phase in range(len(phases)):
        sent(phase)


def fused(n_sp, n_tp, *arrays):
    hidden_in, norm_gain, value_proj = arrays[:3]
    rows, feats = hidden_in.shape
    layers = norm_gain.shape[0]
    piece = value_proj.shape[2]
    blocks = n_sp // n_tp
    channels = blocks * piece
    kinds = 3
    vmem = pl.BlockSpec(memory_space=pltpu.VMEM)
    hbm = pl.BlockSpec(memory_space=pl.ANY)
    low, wide = jnp.bfloat16, jnp.float32
    slots = 4 * blocks + 3 * (rows // ROW_TILE)
    arrays = arrays[:4] + (arrays[4].transpose(1, 0, 2),) + arrays[5:]
    return pl.pallas_call(
        lambda *refs: fused_kernel(n_sp, n_tp, *refs),
        out_shape=jax.ShapeDtypeStruct((rows, feats), low),
        in_specs=[vmem, vmem, hbm, hbm, vmem, vmem, vmem, vmem, hbm],
        out_specs=vmem,
        scratch_shapes=[
            pltpu.VMEM((layers, n_sp, feats, 2 * piece), low),
            pltpu.VMEM((layers, n_sp * piece, feats), low),
            pltpu.VMEM((rows, feats), low),
            pltpu.VMEM((n_tp, blocks, rows, 2 * piece), low),
            pltpu.VMEM((layers, 2, blocks, rows, 2 * piece), low),
            pltpu.VMEM((blocks, rows, 2 * piece), low),
            pltpu.VMEM((layers, blocks, rows, 2 * piece), low),
            pltpu.VMEM((layers, blocks, WIDTH + 1, piece), wide),
            pltpu.VMEM((blocks, HALO + rows, piece), wide),
            pltpu.VMEM((blocks, HALO, piece), low),
            pltpu.VMEM((layers, blocks, HALO, piece), low),
            pltpu.VMEM((blocks, rows, piece), wide),
            pltpu.VMEM((layers, n_tp, rows, channels), low),
            pltpu.VMEM((layers, n_tp, 8, rows), wide),
            pltpu.VMEM((rows, 8), wide),
            pltpu.SemaphoreType.DMA((layers, kinds)),
            pltpu.SemaphoreType.DMA((layers * 2, 2, 3, n_sp)),
            pltpu.SemaphoreType.DMA((layers * 2, 2, n_sp)),
            pltpu.SemaphoreType.DMA((layers, slots)),
            pltpu.SemaphoreType.DMA((layers, slots)),
            pltpu.SemaphoreType.DMA((layers, 3)),
            pltpu.SemaphoreType.DMA((layers, 3)),
        ],
        compiler_params=pltpu.CompilerParams(
            collective_id=0, has_side_effects=True, vmem_limit_bytes=VMEM_BYTES
        ),
    )(*arrays)


def solution(mesh):
    n_sp, n_tp = mesh.shape["sp"], mesh.shape["tp"]
    piece = C // n_sp
    small = n_tp == 4 and GROUPS == n_tp and n_sp == 2 * n_tp and piece % 128 == 0

    def local(*arrays):
        if small and arrays[0].shape[0] % ROW_TILE == 0:
            return fused(n_sp, n_tp, *arrays)
        return on_device(*arrays)

    return jax.shard_map(
        local,
        mesh=mesh,
        in_specs=(
            P("sp", "tp"),
            P(None, "tp"),
            P(None, "tp", "sp"),
            P(None, "tp", "sp"),
            P(None, None, "tp"),
            P(None, "tp"),
            P(None, "tp"),
            P(None, "tp"),
            P(None, "sp", "tp"),
        ),
        out_specs=P("sp", "tp"),
        check_vma=False,
    )
```

```python
import jax
import jax.numpy as jnp
from jax import lax
from jax.experimental import pallas as pl
from jax.experimental.pallas import tpu as pltpu
from jax.sharding import PartitionSpec as P

D = 4096
C = 1024
GROUPS = 4
WIDTH = 31


row_floor = 1e-06
group_floor = 1e-05


def passed_along(value, axis, steps):
    count = lax.axis_size(axis)
    initial, last = (max(0, -steps), min(count, count - steps))
    return lax.ppermute(value, axis, [(source, source + steps) for source in range(initial, last)])


def rms_normed(residual_rows, gain_part):
    wide_rows = residual_rows.astype(jnp.float32)
    squares = lax.psum(jnp.sum(wide_rows * wide_rows, axis=1), "tp")
    scale_rows = lax.rsqrt(squares / D + row_floor)
    return (wide_rows * scale_rows[:, None] * gain_part.astype(jnp.float32)[None, :]).astype(
        jnp.bfloat16
    )


def gated_input(normed_rows, w_value, w_gate):
    numbers = (((0,), (1,)), ((), ()))
    value_part = lax.dot_general(w_value, normed_rows, numbers, preferred_element_type=jnp.float32)
    gate_part = lax.dot_general(w_gate, normed_rows, numbers, preferred_element_type=jnp.float32)
    summed = lax.psum_scatter(
        jnp.stack([value_part, gate_part], axis=1).astype(jnp.bfloat16),
        "tp",
        scatter_dimension=0,
        tiled=True,
    ).astype(jnp.float32)
    return (summed[:, 0] * jax.nn.sigmoid(summed[:, 1])).astype(jnp.bfloat16)


def depthwise(extended, taps_part, bias_part, out_len):
    widened = extended.astype(jnp.float32)
    taps = taps_part.astype(jnp.float32)
    filtered = (
        jnp.zeros((extended.shape[0], out_len), jnp.float32)
        + bias_part.astype(jnp.float32)[:, None]
    )
    for offset in range(WIDTH):
        filtered = filtered + taps[offset][:, None] * widened[:, offset : offset + out_len]
    return filtered


def group_normed(filtered, gain_part, shift_part, group_size):
    channels, out_len = filtered.shape
    grouped = filtered.reshape(channels // group_size, group_size, out_len)
    group_mean = jnp.mean(grouped, axis=1, keepdims=True)
    centered = grouped - group_mean
    group_var = jnp.mean(centered * centered, axis=1, keepdims=True)
    scaled = (centered * lax.rsqrt(group_var + group_floor)).reshape(channels, out_len)
    scaled = (
        scaled * gain_part.astype(jnp.float32)[:, None] + shift_part.astype(jnp.float32)[:, None]
    )
    return jax.nn.silu(scaled).astype(jnp.bfloat16)


def project_out(mixed, w_out):
    return lax.dot_general(
        lax.all_gather(mixed, "tp", axis=0, tiled=True),
        w_out,
        (((0,), (0,)), ((), ())),
        preferred_element_type=jnp.float32,
    )


def on_device(
    hidden_in,
    norm_gain,
    value_proj,
    gate_proj,
    conv_taps,
    conv_bias,
    group_gain,
    group_shift,
    out_proj,
):
    tok_rows = hidden_in.shape[0]
    layers = norm_gain.shape[0]
    reach_back = WIDTH - 1
    group_size = C // GROUPS
    all_value, all_gate, all_out = (
        lax.all_gather(value_proj, "sp", axis=2, tiled=True),
        lax.all_gather(gate_proj, "sp", axis=2, tiled=True),
        lax.all_gather(out_proj, "sp", axis=1, tiled=True),
    )
    residual_rows = hidden_in
    for level in range(layers):
        w_value, w_gate, w_out = (all_value[level], all_gate[level], all_out[level])
        normed_rows = rms_normed(residual_rows, norm_gain[level])
        gated = gated_input(normed_rows, w_value, w_gate)
        before = passed_along(gated[:, tok_rows - reach_back :], "sp", 1)
        extended = jnp.concatenate([before, gated], axis=1)
        out_len = extended.shape[1] - reach_back
        filtered = depthwise(extended, conv_taps[level], conv_bias[level], out_len)
        mixed = group_normed(filtered, group_gain[level], group_shift[level], group_size)
        update = project_out(mixed, w_out)
        kept_rows = residual_rows
        residual_rows = (kept_rows.astype(jnp.float32) + update).astype(jnp.bfloat16)
    return residual_rows


MESH = pl.DeviceIdType.MESH
HALO = 32
ROW_TILE = 256
CONV_TILE = 64
VMEM_BYTES = 62 * 1024 * 1024


def fused_kernel(
    n_sp,
    n_tp,
    hidden_ref,
    norm_ref,
    value_ref,
    gate_ref,
    taps_ref,
    bias_ref,
    ggain_ref,
    gshift_ref,
    out_proj_ref,
    out_ref,
    held,
    w_in,
    w_out,
    scaled,
    part,
    from_core,
    to_chip,
    from_chip,
    taps,
    extended,
    halo_send,
    halo_recv,
    filtered,
    mixed,
    squares,
    scales,
    guest,
    guest_part,
    guest_core,
    guest_out,
    guest_in,
    guest_gated,
    lent,
    guest_sum,
    guest_sums,
    guest_scales,
    load_sem,
    result_sem,
    w_send,
    w_recv,
    t_send,
    t_recv,
    s_send,
    s_recv,
    g_send,
    g_recv,
):
    width, layers = taps_ref.shape[0], taps_ref.shape[1]
    rows, feats = hidden_ref.shape
    piece = value_ref.shape[2]
    blocks = n_sp // n_tp
    channels = blocks * piece
    reach = width - 1
    nz = n_sp // 2
    s = lax.axis_index("sp")
    t = lax.axis_index("tp")
    z, y = s // 2, s % 2
    chip, core = t // 2, t % 2
    core_mate = chip * 2 + (1 - core)
    chip_mate = (1 - chip) * 2 + core
    far_mate = (1 - chip) * 2 + (1 - core)
    across = z * 2 + 1 - y

    taken = pltpu.make_async_copy(hidden_ref, held, load_sem.at[0, 3])
    loads = []
    for level in range(layers):
        for kind, (source, target) in enumerate(
            (
                (value_ref.at[level], w_in.at[level, s, :, pl.ds(0, piece)]),
                (gate_ref.at[level], w_in.at[level, s, :, pl.ds(piece, piece)]),
                (
                    out_proj_ref.at[level],
                    w_out.at[level, pl.ds(pl.multiple_of(s * piece, piece), piece), :],
                ),
            )
        ):
            copy = pltpu.make_async_copy(source, target, load_sem.at[level, kind])
            copy.start()
            loads.append(copy)

    taken.start()
    barrier = pltpu.get_barrier_semaphore()

    def greet(sp_index, tp_index):
        pl.semaphore_signal(barrier, inc=1, device_id=(sp_index, tp_index), device_id_type=MESH)

    up, down = z < nz - 1, z > 0
    corner_up = jnp.logical_and(up, y == 1)
    corner_down = jnp.logical_and(down, y == 0)
    for mate in (core_mate, chip_mate, far_mate):
        greet(s, mate)
    greet(across, t)
    for condition, target in (
        (up, s + 2),
        (down, s - 2),
        (corner_up, s + 1),
        (corner_down, s - 1),
    ):

        @pl.when(condition)
        def _(target=target):
            greet(target, t)

    mates = 4
    for condition in (up, down, corner_up, corner_down):
        mates = mates + condition.astype(jnp.int32)
    pl.semaphore_wait(barrier, mates)

    for copy in loads[:2]:
        copy.wait()

    phases = []
    for level in range(layers):
        phases += [("in", level), ("out", level)]

    def chunk(phase, owner, lot):
        kind, level = phases[phase]
        if kind == "in":
            size = feats // 2
            return w_in.at[level, owner, pl.ds(lot * size, size), :]
        size = piece // 2
        return w_out.at[
            level, pl.ds(pl.multiple_of(owner * piece + lot * size, size), size), :
        ]

    def place_of(owner, way, lot):
        source, column = owner // 2, owner % 2
        if way == 2:
            return 2 * source + lot
        return 2 * nz + (2 * (source + way) + lot) * (1 - (column + y) % 2) + (
            2 * (nz + 1) + way
        ) * ((column + y) % 2)

    def weight_copy(phase, owner, way, lot):
        return pltpu.make_async_remote_copy(
            src_ref=chunk(phase, owner, lot),
            dst_ref=chunk(phase, owner, lot),
            send_sem=w_send.at[phase, place_of(owner, way, lot)],
            recv_sem=w_recv.at[phase, lot, owner],
            device_id=((s + 2, s - 2, across)[way], t),
            device_id_type=MESH,
        )

    def go(phase, owner, way, lot, finish):
        copy = weight_copy(phase, owner, way, lot)
        if finish:
            copy.wait_send()
        else:
            copy.start()

    def come(phase, owner, lot, finish):
        if not finish:
            weight_copy(phase, owner, 2, lot).wait_recv()

    outer = jnp.logical_or(z == 0, z == nz - 1)
    middle = jnp.logical_and(z > 0, z < nz - 1)

    def own_rows(phase, finish=False):
        for lot in (1, 0):
            go(phase, s, 2, lot, finish)

    def own_column(phase, ends=None, finish=False):
        to_end = (z == nz - 2, z == 1)
        to_middle = (z < nz - 2, z > 1)
        conditions = (up, down) if ends is None else to_end if ends else to_middle
        for lot in (0, 1):
            for way, condition in enumerate(conditions):

                @pl.when(condition)
                def _(way=way, lot=lot):
                    go(phase, s, way, lot, finish)

    def turn(phase, finish=False):
        for way, place in enumerate((0, nz - 1)):

            @pl.when(z == place)
            def _(way=way):
                come(phase, across, 1, finish)
                go(phase, across, way, 1, finish)

    def hop(phase, steps, lots=(0, 1), ends=None, finish=False):
        for lot in lots:
            for way, sign in enumerate((-1, 1)):
                source = z + sign * steps
                inside = source >= 0 if way == 0 else source < nz
                inner = source > 0 if way == 0 else source < nz - 1
                onward = up if way == 0 else down
                if phase == 0:
                    onward = z < nz - 2 if way == 0 else z > 1
                    if steps > 1:
                        inside = jnp.logical_and(inside, middle)
                if ends is not None:
                    place = 0 if way == 0 else nz - 1
                    inside = source == place if ends else jnp.logical_and(inside, inner)

                @pl.when(inside)
                def _(way=way, lot=lot, source=source, inner=inner, onward=onward):
                    owner = source * 2 + y
                    come(phase, owner, lot, finish)

                    @pl.when(onward)
                    def _():
                        go(phase, owner, way, lot, finish)

                    if lot == 0:
                        go(phase, owner, 2, lot, finish)
                    else:

                        @pl.when(inner)
                        def _():
                            go(phase, owner, 2, lot, finish)

    def side(phase, steps, finish=False):
        if phase == 0 and steps == nz - 1:
            return
        for way, place in enumerate((0, nz - 1)):
            source = z - steps if way == 0 else z + steps
            onward = up if way == 0 else down
            if phase == 0:
                onward = z < nz - 2 if way == 0 else z > 1

            @pl.when(source == place)
            def _(way=way, place=place, onward=onward):
                owner = place * 2 + 1 - y
                come(phase, owner, 1, finish)

                @pl.when(onward)
                def _():
                    go(phase, owner, way, 1, finish)

    def apart(condition, *steps):
        @pl.when(condition)
        def _():
            for function, *arguments in steps:
                function(*arguments)

    def crossed(phase, source):
        owner = source * 2 + 1 - y
        come(phase, owner, 0, False)

        @pl.when(jnp.logical_and(source > 0, source < nz - 1))
        def _():
            come(phase, owner, 1, False)

    def sent(phase):
        own_rows(phase, True)
        own_column(phase, finish=True)
        turn(phase, True)
        for steps in range(1, nz):
            hop(phase, steps, finish=True)
            side(phase, steps, finish=True)

    def tp_copy(level, slot, source, target, mate, sp_index=None):
        return pltpu.make_async_remote_copy(
            src_ref=source,
            dst_ref=target,
            send_sem=t_send.at[slot],
            recv_sem=t_recv.at[slot],
            device_id=(s if sp_index is None else sp_index, mate),
            device_id_type=MESH,
        )

    tiles = rows // ROW_TILE
    order = tuple(reversed(range(tiles)))

    def prepare(level, tile):
        gain = norm_ref[pl.ds(level, 1), :].astype(jnp.float32)
        ones = jnp.ones((8, feats), jnp.bfloat16)
        numbers = (((1,), (1,)), ((), ()))
        span = pl.ds(tile * ROW_TILE, ROW_TILE)
        wide = held[span, :].astype(jnp.float32)
        scaled[span, :] = (wide * gain).astype(jnp.bfloat16)
        square = wide * wide
        high = square.astype(jnp.bfloat16)
        low = (square - high.astype(jnp.float32)).astype(jnp.bfloat16)
        total = lax.dot_general(ones, high, numbers, preferred_element_type=jnp.float32)
        total = total + lax.dot_general(ones, low, numbers, preferred_element_type=jnp.float32)
        squares[level, t, :, span] = total

    def square_copies(level):
        return [
            pltpu.make_async_remote_copy(
                src_ref=squares.at[level, t],
                dst_ref=squares.at[level, t],
                send_sem=s_send.at[slot],
                recv_sem=s_recv.at[slot],
                device_id=(s, mate),
                device_id_type=MESH,
            )
            for slot, mate in enumerate((core_mate, chip_mate, far_mate))
        ]

    def row_scales(level):
        for copy in square_copies(level):
            copy.wait_send()
            copy.wait_recv()
        total = squares[level, 0]
        for index in range(1, n_tp):
            total = total + squares[level, index]
        scales[...] = lax.rsqrt(total / D + row_floor).T
        if level == 0:
            guest_sum[...] = total

    def core_copy(level, target_chip, block):
        owner = target_chip * 2 + 1 - core
        return tp_copy(
            level,
            target_chip * blocks + block,
            part.at[owner, block],
            from_core.at[level, target_chip, block],
            core_mate,
        )

    base = 2 * blocks

    def chip_copy(level, block):
        return tp_copy(
            level, base + block, to_chip.at[block], from_chip.at[level, block], chip_mate
        )

    def halo_copy(level, block):
        return tp_copy(
            level,
            base + (1 + level) * blocks + block,
            halo_send.at[block],
            halo_recv.at[level, block],
            t,
            s + 1,
        )

    def mixed_copy(level, slot, third):
        owner = (t, t, chip_mate)[slot]
        mate = (core_mate, chip_mate, core_mate)[slot]
        block = mixed.at[level, owner, pl.ds(third * ROW_TILE, ROW_TILE), :]
        return tp_copy(level, base + (1 + layers) * blocks + slot * tiles + third, block, block, mate)

    def target_of(turn_index):
        upper = z // (nz // 2)
        near = z + upper * (nz - 1 - 2 * z)
        pick = (near, 1 - near)[turn_index] if turn_index < 2 else turn_index
        return pick + upper * (nz - 1 - 2 * pick)

    def products(level, target, block):
        @pl.loop(0, tiles)
        def _(tile):
            span = pl.ds(pl.multiple_of(tile * ROW_TILE, ROW_TILE), ROW_TILE)
            part[target, block, span, :] = jnp.dot(
                scaled[span, :],
                w_in[level, target * blocks + block],
                preferred_element_type=jnp.float32,
            ).astype(jnp.bfloat16)

        @pl.when(target % 2 != core)
        def _():
            core_copy(level, target // 2, block).start()

    def contribute(level, target, turned):
        block = 1 - y if turned else y
        if turned:
            crossed(2 * level, target)
        products(level, target, block)

    def pass_on(level, target, turned):
        block = 1 - y if turned else y

        @pl.when(target == chip_mate)
        def _():
            core_copy(level, 1 - chip, block).wait_recv()

            @pl.loop(0, tiles)
            def _(tile):
                span = pl.ds(pl.multiple_of(tile * ROW_TILE, ROW_TILE), ROW_TILE)
                to_chip[block, span, :] = (
                    part[chip_mate, block, span, :].astype(jnp.float32)
                    + from_core[level, 1 - chip, block, span, :].astype(jnp.float32)
                ).astype(jnp.bfloat16)

            chip_copy(level, block).start()

    def gating(level, block):
        core_copy(level, chip, block).wait_recv()
        chip_copy(level, block).wait_recv()

        @pl.loop(0, tiles)
        def _(tile):
            start = pl.multiple_of(tile * ROW_TILE, ROW_TILE)
            span = pl.ds(start, ROW_TILE)
            total = (
                part[t, block, span, :].astype(jnp.float32)
                + from_core[level, chip, block, span, :].astype(jnp.float32)
                + from_chip[level, block, span, :].astype(jnp.float32)
            ) * scales[span, 0:1]
            gated = (total[:, :piece] * jax.nn.sigmoid(total[:, piece:])).astype(jnp.bfloat16)
            extended[block, pl.ds(HALO + start, ROW_TILE), :] = gated.astype(jnp.float32)

        halo_send[block] = extended[block, pl.ds(rows, HALO), :].astype(jnp.bfloat16)

        @pl.when(s < n_sp - 1)
        def _():
            halo_copy(level, block).start()

    upper_half = z // (nz // 2)
    guest_chip = 1 - upper_half
    host = jnp.logical_and(middle, chip == guest_chip)
    feeder = jnp.logical_and(middle, chip != guest_chip)
    lender = jnp.logical_and(outer, chip == guest_chip)
    keeper = jnp.logical_and(outer, chip != guest_chip)

    def guest_copy(kind, third):
        span = pl.ds(third * ROW_TILE, ROW_TILE)
        inward = s + 2 - 4 * upper_half
        outward = s - 2 + 4 * upper_half
        source, target, place, mate = (
            (scaled.at[span, :], guest.at[span, :], inward, t),
            (guest_part.at[1, third], guest_core.at[third], s, core_mate),
            (guest_out.at[third], guest_in.at[third], s, chip_mate),
            (guest_gated.at[third], lent.at[third], outward, t),
            (guest_sum, guest_sums, inward, t),
        )[kind]
        return pltpu.make_async_remote_copy(
            src_ref=source,
            dst_ref=target,
            send_sem=g_send.at[kind * tiles + third],
            recv_sem=g_recv.at[kind * tiles + third],
            device_id=(place, mate),
            device_id_type=MESH,
        )

    def guest_start():
        guest_copy(4, 0).start()
        for third in order[:-1]:
            guest_copy(0, third).start()
        own_column(1)
        guest_copy(0, order[-1]).start()

    def guest_left():
        guest_copy(4, 0).wait_send()
        for third in order:
            guest_copy(0, third).wait_send()

    def guest_scale():
        guest_copy(4, 0).wait_recv()
        guest_scales[...] = lax.rsqrt(guest_sums[...] / D + row_floor).T

    def guest_products(third):
        guest_copy(0, third).wait_recv()
        span = pl.ds(third * ROW_TILE, ROW_TILE)

        for which in (1, 0):
            owner = (guest_chip * 2 + (core if which == 0 else 1 - core)) * blocks

            @pl.loop(0, blocks)
            def _(block, which=which, owner=owner):
                guest_part[which, third, block] = jnp.dot(
                    guest[span, :], w_in[0, owner + block], preferred_element_type=jnp.float32
                ).astype(jnp.bfloat16)

            if which == 1:
                guest_copy(1, third).start()

    def guest_pass(third):
        guest_copy(1, third).wait_recv()
        guest_out[third] = (
            guest_part[0, third].astype(jnp.float32) + guest_core[third].astype(jnp.float32)
        ).astype(jnp.bfloat16)
        guest_copy(2, third).start()

    def guest_gate(third):
        guest_copy(1, third).wait_recv()
        guest_copy(2, third).wait_recv()
        span = pl.ds(third * ROW_TILE, ROW_TILE)
        for block in range(blocks):
            total = (
                guest_part[0, third, block].astype(jnp.float32)
                + guest_core[third, block].astype(jnp.float32)
                + guest_in[third, block].astype(jnp.float32)
            ) * guest_scales[span, 0:1]
            guest_gated[third, block] = (
                total[:, :piece] * jax.nn.sigmoid(total[:, piece:])
            ).astype(jnp.bfloat16)
        guest_copy(3, third).start()

    def lend(third):
        guest_copy(3, third).wait_recv()
        for block in range(blocks):
            extended[block, pl.ds(HALO + third * ROW_TILE, ROW_TILE), :] = lent[
                third, block
            ].astype(jnp.float32)
            if third == tiles - 1:
                halo_send[block] = lent[third, block, ROW_TILE - HALO :, :]

                @pl.when(s < n_sp - 1)
                def _(block=block):
                    halo_copy(0, block).start()

    def guest_settle():
        for third in order:
            apart(middle, (guest_sent, 1, third))
            apart(feeder, (guest_sent, 2, third))
            apart(host, (guest_sent, 3, third))

    def guest_sent(kind, third):
        guest_copy(kind, third).wait_send()

    per_part = ROW_TILE // CONV_TILE

    def convolve(level, block, third):
        bias = taps[level, block, pl.ds(width, 1), :]
        weights = taps[level, block]

        @pl.loop(third * per_part, (third + 1) * per_part)
        def _(tile):
            start = pl.multiple_of(tile * CONV_TILE, CONV_TILE)
            window = extended[block, pl.ds(start, CONV_TILE + HALO), :]
            total = jnp.zeros((CONV_TILE, piece), jnp.float32) + bias
            for offset in range(width):
                low = HALO - reach + offset
                total = total + weights[offset : offset + 1, :] * window[low : low + CONV_TILE]
            filtered[block, pl.ds(start, CONV_TILE), :] = total

    def first_rows(level, block):
        @pl.when(s > 0)
        def _():
            halo_copy(level, block).wait_recv()
            extended[block, pl.ds(0, HALO), :] = halo_recv[level, block].astype(jnp.float32)

        @pl.when(s == 0)
        def _():
            extended[block, pl.ds(0, HALO), :] = jnp.zeros((HALO, piece), jnp.float32)

    def normalise(level, third):
        ggain = ggain_ref[pl.ds(level, 1), :].astype(jnp.float32)
        gshift = gshift_ref[pl.ds(level, 1), :].astype(jnp.float32)

        @pl.loop(third * per_part, (third + 1) * per_part)
        def _(tile):
            span = pl.ds(pl.multiple_of(tile * CONV_TILE, CONV_TILE), CONV_TILE)
            pieces = [filtered[block, span, :] for block in range(blocks)]
            mean = sum(jnp.sum(value, axis=1, keepdims=True) for value in pieces) / channels
            pieces = [value - mean for value in pieces]
            var = sum(jnp.sum(value * value, axis=1, keepdims=True) for value in pieces) / channels
            factor = lax.rsqrt(var + group_floor)
            for block in range(blocks):
                lanes = slice(block * piece, (block + 1) * piece)
                normed = pieces[block] * factor * ggain[:, lanes] + gshift[:, lanes]
                mixed[level, t, span, lanes] = (normed * jax.nn.sigmoid(normed)).astype(
                    jnp.bfloat16
                )

        mixed_copy(level, 1, third).start()
        mixed_copy(level, 0, third).start()

    def relay(level, third):
        mixed_copy(level, 1, third).wait_recv()
        mixed_copy(level, 2, third).start()

    def projecting(level, third):
        mixed_copy(level, 0, third).wait_recv()
        mixed_copy(level, 2, third).wait_recv()
        span = pl.ds(third * ROW_TILE, ROW_TILE)
        total = held[span, :].astype(jnp.float32)
        for owner in range(n_tp):
            total = total + jnp.dot(
                mixed[level, owner, span, :],
                w_out[level, pl.ds(owner * channels, channels), :],
                preferred_element_type=jnp.float32,
            )
        held[span, :] = total.astype(jnp.bfloat16)
        if level + 1 < layers:
            prepare(level + 1, third)
        else:
            result_copy(third).start()

    def result_copy(third):
        span = pl.ds(third * ROW_TILE, ROW_TILE)
        return pltpu.make_async_copy(held.at[span, :], out_ref.at[span, :], result_sem.at[third])

    def settle(level):
        for target_chip in range(2):
            used = middle if level == 0 else z >= 0

            @pl.when(jnp.logical_or(used, target_chip != guest_chip))
            def _(target_chip=target_chip):
                for block in range(blocks):
                    core_copy(level, target_chip, block).wait_send()

        passed = jnp.logical_or(middle, lender) if level == 0 else z >= 0

        @pl.when(passed)
        def _():
            for block in range(blocks):
                chip_copy(level, block).wait_send()

        for slot in range(3):
            for third in order:
                mixed_copy(level, slot, third).wait_send()

        @pl.when(s < n_sp - 1)
        def _():
            for block in range(blocks):
                halo_copy(level, block).wait_send()

    own_rows(0)
    own_column(0)
    for copy in loads[2:]:
        copy.wait()
    for level in range(layers):
        for block in range(blocks):
            lanes = slice(block * piece, (block + 1) * piece)
            taps[level, block, 0:width, :] = taps_ref[:, level, lanes].astype(jnp.float32)
            taps[level, block, width : width + 1, :] = bias_ref[level : level + 1, lanes].astype(
                jnp.float32
            )
    taken.wait()
    for tile in range(tiles):
        prepare(0, tile)
    for copy in square_copies(0):
        copy.start()
    row_scales(0)
    goals = [target_of(turn_index) for turn_index in range(n_tp)]

    def late(third):
        for block in (y, 1 - y):
            convolve(0, block, third)
        normalise(0, third)

    def end_start():
        turn(0)
        guest_start()
        contribute(0, goals[0], 0)
        hop(0, 1)
        own_rows(1)
        contribute(0, goals[1], 0)
        contribute(0, goals[0], 1)
        pass_on(0, goals[0], 0)
        pass_on(0, goals[1], 0)
        contribute(0, goals[1], 1)
        pass_on(0, goals[0], 1)
        pass_on(0, goals[1], 1)
        turn(1)
        hop(1, 1)
        own_rows(2)
        apart(
            keeper,
            (gating, 0, y),
            (gating, 0, 1 - y),
        )
        hop(1, 2)
        hop(2, 1)
        apart(
            keeper,
            *((convolve, 0, y, third) for third in order[:-1]),
            *(
                step
                for third in order[:-1]
                for step in ((convolve, 0, 1 - y, third), (normalise, 0, third))
            ),
        )
        apart(lender, (lend, order[0]))
        own_column(2)
        turn(2)
        apart(lender, (lend, order[1]), (late, order[0]))
        hop(1, 3)
        own_column(3)
        apart(lender, (lend, order[2]), (late, order[1]))
        hop(2, 2, (0,))

    def middle_start():
        for phase in range(1, len(phases)):
            own_column(phase, True)
        contribute(0, goals[0], 0)
        hop(0, 1)
        contribute(0, goals[1], 0)
        contribute(0, goals[2], 0)
        contribute(0, goals[0], 1)
        pass_on(0, goals[0], 0)
        side(0, 1)
        hop(0, 2)
        own_rows(1)
        own_column(1, False)
        pass_on(0, goals[1], 0)
        pass_on(0, goals[2], 0)
        contribute(0, goals[3], 0)
        pass_on(0, goals[0], 1)
        contribute(0, goals[1], 1)
        pass_on(0, goals[3], 0)
        pass_on(0, goals[1], 1)
        contribute(0, goals[2], 1)
        side(0, 2)
        pass_on(0, goals[2], 1)
        contribute(0, goals[3], 1)
        own_column(2, False)
        guest_scale()
        guest_products(order[0])
        pass_on(0, goals[3], 1)
        hop(1, 1, (0, 1), False)
        apart(feeder, (guest_pass, order[0]))
        guest_products(order[1])
        gating(0, y)
        for third in order[:-1]:
            convolve(0, y, third)
        hop(2, 1, (0,), False)
        apart(feeder, (guest_pass, order[1]))
        gating(0, 1 - y)
        hop(1, 1, (0, 1), True)
        hop(2, 1, (1,), False)
        apart(host, (guest_gate, order[0]))
        for third in order[:-1]:
            convolve(0, 1 - y, third)
            normalise(0, third)
        hop(1, 2)
        own_rows(2)
        apart(host, (guest_gate, order[1]))
        guest_products(order[2])
        apart(feeder, (guest_pass, order[2]))
        side(1, 1)
        side(1, 2)
        apart(host, (guest_gate, order[2]))

    apart(outer, (end_start,))
    apart(middle, (middle_start,))
    end = outer.astype(jnp.int32)
    for level in range(layers):
        first, second = 2 * level, 2 * level + 1
        last = level == layers - 1
        targets = [target_of(turn_index) for turn_index in range(n_tp)]
        third_target = targets[2] * end + targets[3] * (1 - end)
        if level > 0:
            contribute(level, targets[0], 0)
            contribute(level, targets[1], 0)
            apart(middle, (contribute, level, targets[2], 0))
            contribute(level, targets[0], 1)
            pass_on(level, targets[0], 0)
            apart(outer, (hop, first, 2, (1,)))
            pass_on(level, targets[1], 0)
            apart(middle, (pass_on, level, targets[2], 0))
            contribute(level, third_target, 0)
            pass_on(level, targets[0], 1)
            contribute(level, targets[1], 1)
            apart(
                outer,
                (hop, first, 3),
                (own_rows, second),
                (hop, second, 1),
                (contribute, level, targets[3], 0),
            )
            pass_on(level, third_target, 0)
            pass_on(level, targets[1], 1)
            contribute(level, targets[2], 1)
            apart(outer, (pass_on, level, targets[3], 0))
            pass_on(level, targets[2], 1)
            apart(outer, (side, first, nz - 1))
            apart(middle, (side, first, nz - 2), (own_rows, second), (own_column, second, False))
            contribute(level, targets[3], 1)
            pass_on(level, targets[3], 1)
            apart(outer, (turn, second))
            apart(middle, (hop, second, 1))
            row_scales(level)
            gating(level, y)
            for third in order[:-1]:
                convolve(level, y, third)
            apart(outer, (hop, second, 2, (0,)))
            gating(level, 1 - y)
            apart(middle, (hop, second, 2))
            for third in order[:-1]:
                convolve(level, 1 - y, third)
                normalise(level, third)
                if third == order[0]:
                    apart(outer, (hop, second, 2, (1,)), (hop, second, 3, (0,)))
            apart(middle, (side, second, 1), (side, second, 2))
        for block in (y, 1 - y):
            first_rows(level, block)
            convolve(level, block, order[-1])
        normalise(level, order[-1])
        relay(level, order[0])
        if level > 0:
            apart(outer, (hop, second, 3, (1,)), (side, second, nz - 1))
        else:
            apart(outer, (guest_left,), (side, second, nz - 1))
        if not last:
            apart(middle, (hop, first + 2, 1, (0,), True))
        for source in range(nz):
            crossed(second, source)
        if not last:
            apart(middle, (hop, first + 2, 1, (1,), True))
        for index in range(1, tiles):
            relay(level, order[index])
            projecting(level, order[index - 1])
        projecting(level, order[-1])
        if not last:
            for copy in square_copies(level + 1):
                copy.start()
            apart(middle, (side, first + 2, 1), (hop, first + 2, 2))
        settle(level)
    guest_settle()
    for phase in range(len(phases)):
        sent(phase)
    for third in order:
        result_copy(third).wait()


def fused(n_sp, n_tp, *arrays):
    hidden_in, norm_gain, value_proj = arrays[:3]
    rows, feats = hidden_in.shape
    layers = norm_gain.shape[0]
    piece = value_proj.shape[2]
    blocks = n_sp // n_tp
    channels = blocks * piece
    kinds = 4
    tiles = rows // ROW_TILE
    vmem = pl.BlockSpec(memory_space=pltpu.VMEM)
    hbm = pl.BlockSpec(memory_space=pltpu.HBM)
    low, wide = jnp.bfloat16, jnp.float32
    slots = (3 + layers) * blocks + 3 * (rows // ROW_TILE)
    arrays = arrays[:4] + (arrays[4].transpose(1, 0, 2),) + arrays[5:]
    return pl.pallas_call(
        lambda *refs: fused_kernel(n_sp, n_tp, *refs),
        out_shape=jax.ShapeDtypeStruct((rows, feats), low),
        in_specs=[hbm, vmem, hbm, hbm, vmem, vmem, vmem, vmem, hbm],
        out_specs=hbm,
        scratch_shapes=[
            pltpu.VMEM((rows, feats), low),
            pltpu.VMEM((layers, n_sp, feats, 2 * piece), low),
            pltpu.VMEM((layers, n_sp * piece, feats), low),
            pltpu.VMEM((rows, feats), low),
            pltpu.VMEM((n_tp, blocks, rows, 2 * piece), low),
            pltpu.VMEM((layers, 2, blocks, rows, 2 * piece), low),
            pltpu.VMEM((blocks, rows, 2 * piece), low),
            pltpu.VMEM((layers, blocks, rows, 2 * piece), low),
            pltpu.VMEM((layers, blocks, WIDTH + 1, piece), wide),
            pltpu.VMEM((blocks, HALO + rows, piece), wide),
            pltpu.VMEM((blocks, HALO, piece), low),
            pltpu.VMEM((layers, blocks, HALO, piece), low),
            pltpu.VMEM((blocks, rows, piece), wide),
            pltpu.VMEM((layers, n_tp, rows, channels), low),
            pltpu.VMEM((layers, n_tp, 8, rows), wide),
            pltpu.VMEM((rows, 8), wide),
            pltpu.VMEM((rows, feats), low),
            pltpu.VMEM((2, tiles, blocks, ROW_TILE, 2 * piece), low),
            pltpu.VMEM((tiles, blocks, ROW_TILE, 2 * piece), low),
            pltpu.VMEM((tiles, blocks, ROW_TILE, 2 * piece), low),
            pltpu.VMEM((tiles, blocks, ROW_TILE, 2 * piece), low),
            pltpu.VMEM((tiles, blocks, ROW_TILE, piece), low),
            pltpu.VMEM((tiles, blocks, ROW_TILE, piece), low),
            pltpu.VMEM((8, rows), wide),
            pltpu.VMEM((8, rows), wide),
            pltpu.VMEM((rows, 8), wide),
            pltpu.SemaphoreType.DMA((layers, kinds)),
            pltpu.SemaphoreType.DMA((rows // ROW_TILE,)),
            pltpu.SemaphoreType.DMA((layers * 2, 2 * n_sp + 4)),
            pltpu.SemaphoreType.DMA((layers * 2, 2, n_sp)),
            pltpu.SemaphoreType.DMA((slots,)),
            pltpu.SemaphoreType.DMA((slots,)),
            pltpu.SemaphoreType.DMA((3,)),
            pltpu.SemaphoreType.DMA((3,)),
            pltpu.SemaphoreType.DMA((4 * tiles + 1,)),
            pltpu.SemaphoreType.DMA((4 * tiles + 1,)),
        ],
        compiler_params=pltpu.CompilerParams(
            collective_id=0, has_side_effects=True, vmem_limit_bytes=VMEM_BYTES
        ),
    )(*arrays)


def solution(mesh):
    n_sp, n_tp = mesh.shape["sp"], mesh.shape["tp"]
    piece = C // n_sp
    small = n_tp == 4 and GROUPS == n_tp and n_sp == 8 and piece % 128 == 0

    def local(*arrays):
        if small and arrays[0].shape[0] % ROW_TILE == 0:
            return fused(n_sp, n_tp, *arrays)
        return on_device(*arrays)

    return jax.shard_map(
        local,
        mesh=mesh,
        in_specs=(
            P("sp", "tp"),
            P(None, "tp"),
            P(None, "tp", "sp"),
            P(None, "tp", "sp"),
            P(None, None, "tp"),
            P(None, "tp"),
            P(None, "tp"),
            P(None, "tp"),
            P(None, "sp", "tp"),
        ),
        out_specs=P("sp", "tp"),
        check_vma=False,
    )
```

```python
import jax
import jax.numpy as jnp
from jax import lax
from jax.experimental import pallas as pl
from jax.experimental.pallas import tpu as pltpu
from jax.sharding import PartitionSpec as P

D = 4096
C = 1024
GROUPS = 4
WIDTH = 31


row_floor = 1e-06
group_floor = 1e-05


def passed_along(value, axis, steps):
    count = lax.axis_size(axis)
    initial, last = (max(0, -steps), min(count, count - steps))
    return lax.ppermute(value, axis, [(source, source + steps) for source in range(initial, last)])


def rms_normed(residual_rows, gain_part):
    wide_rows = residual_rows.astype(jnp.float32)
    squares = lax.psum(jnp.sum(wide_rows * wide_rows, axis=1), "tp")
    scale_rows = lax.rsqrt(squares / D + row_floor)
    return (wide_rows * scale_rows[:, None] * gain_part.astype(jnp.float32)[None, :]).astype(
        jnp.bfloat16
    )


def gated_input(normed_rows, w_value, w_gate):
    numbers = (((0,), (1,)), ((), ()))
    value_part = lax.dot_general(w_value, normed_rows, numbers, preferred_element_type=jnp.float32)
    gate_part = lax.dot_general(w_gate, normed_rows, numbers, preferred_element_type=jnp.float32)
    summed = lax.psum_scatter(
        jnp.stack([value_part, gate_part], axis=1).astype(jnp.bfloat16),
        "tp",
        scatter_dimension=0,
        tiled=True,
    ).astype(jnp.float32)
    return (summed[:, 0] * jax.nn.sigmoid(summed[:, 1])).astype(jnp.bfloat16)


def depthwise(extended, taps_part, bias_part, out_len):
    widened = extended.astype(jnp.float32)
    taps = taps_part.astype(jnp.float32)
    filtered = (
        jnp.zeros((extended.shape[0], out_len), jnp.float32)
        + bias_part.astype(jnp.float32)[:, None]
    )
    for offset in range(WIDTH):
        filtered = filtered + taps[offset][:, None] * widened[:, offset : offset + out_len]
    return filtered


def group_normed(filtered, gain_part, shift_part, group_size):
    channels, out_len = filtered.shape
    grouped = filtered.reshape(channels // group_size, group_size, out_len)
    group_mean = jnp.mean(grouped, axis=1, keepdims=True)
    centered = grouped - group_mean
    group_var = jnp.mean(centered * centered, axis=1, keepdims=True)
    scaled = (centered * lax.rsqrt(group_var + group_floor)).reshape(channels, out_len)
    scaled = (
        scaled * gain_part.astype(jnp.float32)[:, None] + shift_part.astype(jnp.float32)[:, None]
    )
    return jax.nn.silu(scaled).astype(jnp.bfloat16)


def project_out(mixed, w_out):
    return lax.dot_general(
        lax.all_gather(mixed, "tp", axis=0, tiled=True),
        w_out,
        (((0,), (0,)), ((), ())),
        preferred_element_type=jnp.float32,
    )


def on_device(
    hidden_in,
    norm_gain,
    value_proj,
    gate_proj,
    conv_taps,
    conv_bias,
    group_gain,
    group_shift,
    out_proj,
):
    tok_rows = hidden_in.shape[0]
    layers = norm_gain.shape[0]
    reach_back = WIDTH - 1
    group_size = C // GROUPS
    all_value, all_gate, all_out = (
        lax.all_gather(value_proj, "sp", axis=2, tiled=True),
        lax.all_gather(gate_proj, "sp", axis=2, tiled=True),
        lax.all_gather(out_proj, "sp", axis=1, tiled=True),
    )
    residual_rows = hidden_in
    for level in range(layers):
        w_value, w_gate, w_out = (all_value[level], all_gate[level], all_out[level])
        normed_rows = rms_normed(residual_rows, norm_gain[level])
        gated = gated_input(normed_rows, w_value, w_gate)
        before = passed_along(gated[:, tok_rows - reach_back :], "sp", 1)
        extended = jnp.concatenate([before, gated], axis=1)
        out_len = extended.shape[1] - reach_back
        filtered = depthwise(extended, conv_taps[level], conv_bias[level], out_len)
        mixed = group_normed(filtered, group_gain[level], group_shift[level], group_size)
        update = project_out(mixed, w_out)
        kept_rows = residual_rows
        residual_rows = (kept_rows.astype(jnp.float32) + update).astype(jnp.bfloat16)
    return residual_rows


MESH = pl.DeviceIdType.MESH
HALO = 32
ROW_TILE = 256
CONV_TILE = 64
VMEM_BYTES = 62 * 1024 * 1024


def fused_kernel(
    n_sp,
    n_tp,
    hidden_ref,
    norm_ref,
    value_ref,
    gate_ref,
    taps_ref,
    bias_ref,
    ggain_ref,
    gshift_ref,
    out_proj_ref,
    out_ref,
    held,
    w_in,
    w_out,
    scaled,
    part,
    from_core,
    to_chip,
    from_chip,
    taps,
    extended,
    halo_send,
    halo_recv,
    filtered,
    mixed,
    squares,
    scales,
    guest,
    guest_part,
    guest_core,
    guest_out,
    guest_in,
    guest_gated,
    lent,
    guest_sum,
    guest_sums,
    guest_scales,
    load_sem,
    result_sem,
    w_send,
    w_recv,
    t_send,
    t_recv,
    s_send,
    s_recv,
    g_send,
    g_recv,
):
    width, layers = taps_ref.shape[0], taps_ref.shape[1]
    rows, feats = hidden_ref.shape
    piece = value_ref.shape[2]
    blocks = n_sp // n_tp
    channels = blocks * piece
    reach = width - 1
    nz = n_sp // 2
    s = lax.axis_index("sp")
    t = lax.axis_index("tp")
    z, y = s // 2, s % 2
    chip, core = t // 2, t % 2
    core_mate = chip * 2 + (1 - core)
    chip_mate = (1 - chip) * 2 + core
    far_mate = (1 - chip) * 2 + (1 - core)
    across = z * 2 + 1 - y

    taken = pltpu.make_async_copy(hidden_ref, held, load_sem.at[0, 3])
    loads = []
    for level in range(layers):
        for kind, (source, target) in enumerate(
            (
                (value_ref.at[level], w_in.at[level, s, :, pl.ds(0, piece)]),
                (gate_ref.at[level], w_in.at[level, s, :, pl.ds(piece, piece)]),
                (
                    out_proj_ref.at[level],
                    w_out.at[level, pl.ds(pl.multiple_of(s * piece, piece), piece), :],
                ),
            )
        ):
            copy = pltpu.make_async_copy(source, target, load_sem.at[level, kind])
            copy.start()
            loads.append(copy)

    taken.start()
    barrier = pltpu.get_barrier_semaphore()

    def greet(sp_index, tp_index):
        pl.semaphore_signal(barrier, inc=1, device_id=(sp_index, tp_index), device_id_type=MESH)

    up, down = z < nz - 1, z > 0
    corner_up = jnp.logical_and(up, y == 1)
    corner_down = jnp.logical_and(down, y == 0)
    for mate in (core_mate, chip_mate, far_mate):
        greet(s, mate)
    greet(across, t)
    for condition, target in (
        (up, s + 2),
        (down, s - 2),
        (corner_up, s + 1),
        (corner_down, s - 1),
    ):

        @pl.when(condition)
        def _(target=target):
            greet(target, t)

    mates = 4
    for condition in (up, down, corner_up, corner_down):
        mates = mates + condition.astype(jnp.int32)
    pl.semaphore_wait(barrier, mates)

    for copy in loads[:2]:
        copy.wait()

    phases = []
    for level in range(layers):
        phases += [("in", level), ("out", level)]

    def chunk(phase, owner, lot):
        kind, level = phases[phase]
        if kind == "in":
            size = feats // 2
            return w_in.at[level, owner, pl.ds(lot * size, size), :]
        size = piece // 2
        return w_out.at[
            level, pl.ds(pl.multiple_of(owner * piece + lot * size, size), size), :
        ]

    def place_of(owner, way, lot):
        source, column = owner // 2, owner % 2
        if way == 2:
            return 2 * source + lot
        return 2 * nz + (2 * (source + way) + lot) * (1 - (column + y) % 2) + (
            2 * (nz + 1) + way
        ) * ((column + y) % 2)

    def weight_copy(phase, owner, way, lot):
        return pltpu.make_async_remote_copy(
            src_ref=chunk(phase, owner, lot),
            dst_ref=chunk(phase, owner, lot),
            send_sem=w_send.at[phase, place_of(owner, way, lot)],
            recv_sem=w_recv.at[phase, lot, owner],
            device_id=((s + 2, s - 2, across)[way], t),
            device_id_type=MESH,
        )

    def go(phase, owner, way, lot, finish):
        copy = weight_copy(phase, owner, way, lot)
        if finish:
            copy.wait_send()
        else:
            copy.start()

    def come(phase, owner, lot, finish):
        if not finish:
            weight_copy(phase, owner, 2, lot).wait_recv()

    outer = jnp.logical_or(z == 0, z == nz - 1)
    middle = jnp.logical_and(z > 0, z < nz - 1)

    def own_rows(phase, finish=False):
        for lot in (1, 0):
            go(phase, s, 2, lot, finish)

    def own_column(phase, ends=None, finish=False):
        to_end = (z == nz - 2, z == 1)
        to_middle = (z < nz - 2, z > 1)
        conditions = (up, down) if ends is None else to_end if ends else to_middle
        for lot in (0, 1):
            for way, condition in enumerate(conditions):

                @pl.when(condition)
                def _(way=way, lot=lot):
                    go(phase, s, way, lot, finish)

    def turn(phase, finish=False):
        for way, place in enumerate((0, nz - 1)):

            @pl.when(z == place)
            def _(way=way):
                come(phase, across, 1, finish)
                go(phase, across, way, 1, finish)

    def hop(phase, steps, lots=(0, 1), ends=None, finish=False):
        for lot in lots:
            for way, sign in enumerate((-1, 1)):
                source = z + sign * steps
                inside = source >= 0 if way == 0 else source < nz
                inner = source > 0 if way == 0 else source < nz - 1
                onward = up if way == 0 else down
                if phase == 0:
                    onward = z < nz - 2 if way == 0 else z > 1
                    if steps > 1:
                        inside = jnp.logical_and(inside, middle)
                if ends is not None:
                    place = 0 if way == 0 else nz - 1
                    inside = source == place if ends else jnp.logical_and(inside, inner)

                @pl.when(inside)
                def _(way=way, lot=lot, source=source, inner=inner, onward=onward):
                    owner = source * 2 + y
                    come(phase, owner, lot, finish)

                    @pl.when(onward)
                    def _():
                        go(phase, owner, way, lot, finish)

                    if lot == 0:
                        go(phase, owner, 2, lot, finish)
                    else:

                        @pl.when(inner)
                        def _():
                            go(phase, owner, 2, lot, finish)

    def side(phase, steps, finish=False):
        if phase == 0 and steps == nz - 1:
            return
        for way, place in enumerate((0, nz - 1)):
            source = z - steps if way == 0 else z + steps
            onward = up if way == 0 else down
            if phase == 0:
                onward = z < nz - 2 if way == 0 else z > 1

            @pl.when(source == place)
            def _(way=way, place=place, onward=onward):
                owner = place * 2 + 1 - y
                come(phase, owner, 1, finish)

                @pl.when(onward)
                def _():
                    go(phase, owner, way, 1, finish)

    def apart(condition, *steps):
        @pl.when(condition)
        def _():
            for function, *arguments in steps:
                function(*arguments)

    def crossed(phase, source):
        owner = source * 2 + 1 - y
        come(phase, owner, 0, False)

        @pl.when(jnp.logical_and(source > 0, source < nz - 1))
        def _():
            come(phase, owner, 1, False)

    def sent(phase):
        own_rows(phase, True)
        own_column(phase, finish=True)
        turn(phase, True)
        for steps in range(1, nz):
            hop(phase, steps, finish=True)
            side(phase, steps, finish=True)

    def tp_copy(level, slot, source, target, mate, sp_index=None):
        return pltpu.make_async_remote_copy(
            src_ref=source,
            dst_ref=target,
            send_sem=t_send.at[slot],
            recv_sem=t_recv.at[slot],
            device_id=(s if sp_index is None else sp_index, mate),
            device_id_type=MESH,
        )

    tiles = rows // ROW_TILE
    order = tuple(reversed(range(tiles)))

    def prepare(level, tile):
        gain = norm_ref[pl.ds(level, 1), :].astype(jnp.float32)
        ones = jnp.ones((8, feats), jnp.bfloat16)
        numbers = (((1,), (1,)), ((), ()))
        span = pl.ds(tile * ROW_TILE, ROW_TILE)
        wide = held[span, :].astype(jnp.float32)
        scaled[span, :] = (wide * gain).astype(jnp.bfloat16)
        square = wide * wide
        high = square.astype(jnp.bfloat16)
        low = (square - high.astype(jnp.float32)).astype(jnp.bfloat16)
        total = lax.dot_general(ones, high, numbers, preferred_element_type=jnp.float32)
        total = total + lax.dot_general(ones, low, numbers, preferred_element_type=jnp.float32)
        squares[level, t, :, span] = total

    def square_copies(level):
        return [
            pltpu.make_async_remote_copy(
                src_ref=squares.at[level, t],
                dst_ref=squares.at[level, t],
                send_sem=s_send.at[slot],
                recv_sem=s_recv.at[slot],
                device_id=(s, mate),
                device_id_type=MESH,
            )
            for slot, mate in enumerate((core_mate, chip_mate, far_mate))
        ]

    def row_scales(level):
        for copy in square_copies(level):
            copy.wait_send()
            copy.wait_recv()
        total = squares[level, 0]
        for index in range(1, n_tp):
            total = total + squares[level, index]
        scales[...] = lax.rsqrt(total / D + row_floor).T
        if level == 0:
            guest_sum[...] = total

    def rows_of(third):
        return pl.ds(pl.multiple_of(third * ROW_TILE, ROW_TILE), ROW_TILE)

    def core_copy(level, target_chip, block, third):
        owner = target_chip * 2 + 1 - core
        return tp_copy(
            level,
            (target_chip * blocks + block) * tiles + third,
            part.at[owner, block, rows_of(third), :],
            from_core.at[level, target_chip, block, rows_of(third), :],
            core_mate,
        )

    base = 3 * blocks * tiles - blocks

    def chip_copy(level, block, third):
        return tp_copy(
            level,
            (2 * blocks + block) * tiles + third,
            to_chip.at[block, rows_of(third), :],
            from_chip.at[level, block, rows_of(third), :],
            chip_mate,
        )

    def halo_copy(level, block):
        return tp_copy(
            level,
            base + (1 + level) * blocks + block,
            halo_send.at[block],
            halo_recv.at[level, block],
            t,
            s + 1,
        )

    def mixed_copy(level, slot, third):
        owner = (t, t, chip_mate)[slot]
        mate = (core_mate, chip_mate, core_mate)[slot]
        block = mixed.at[level, owner, pl.ds(third * ROW_TILE, ROW_TILE), :]
        return tp_copy(level, base + (1 + layers) * blocks + slot * tiles + third, block, block, mate)

    def target_of(turn_index):
        upper = z // (nz // 2)
        near = z + upper * (nz - 1 - 2 * z)
        pick = (near, 1 - near)[turn_index] if turn_index < 2 else turn_index
        return pick + upper * (nz - 1 - 2 * pick)

    def products(level, target, block):
        @pl.loop(0, tiles)
        def _(step):
            third = tiles - 1 - step
            span = rows_of(third)
            part[target, block, span, :] = jnp.dot(
                scaled[span, :],
                w_in[level, target * blocks + block],
                preferred_element_type=jnp.float32,
            ).astype(jnp.bfloat16)

            @pl.when(target % 2 != core)
            def _():
                core_copy(level, target // 2, block, third).start()

    def contribute(level, target, turned):
        block = 1 - y if turned else y
        if turned:
            crossed(2 * level, target)
        products(level, target, block)

    def pass_on(level, target, turned):
        block = 1 - y if turned else y

        @pl.when(target == chip_mate)
        def _():
            @pl.loop(0, tiles)
            def _(step):
                third = tiles - 1 - step
                span = rows_of(third)
                core_copy(level, 1 - chip, block, third).wait_recv()
                to_chip[block, span, :] = (
                    part[chip_mate, block, span, :].astype(jnp.float32)
                    + from_core[level, 1 - chip, block, span, :].astype(jnp.float32)
                ).astype(jnp.bfloat16)
                chip_copy(level, block, third).start()

    def gate(level, block, third):
        core_copy(level, chip, block, third).wait_recv()
        chip_copy(level, block, third).wait_recv()
        span = rows_of(third)
        total = (
            part[t, block, span, :].astype(jnp.float32)
            + from_core[level, chip, block, span, :].astype(jnp.float32)
            + from_chip[level, block, span, :].astype(jnp.float32)
        ) * scales[span, 0:1]
        gated = (total[:, :piece] * jax.nn.sigmoid(total[:, piece:])).astype(jnp.bfloat16)
        extended[block, pl.ds(HALO + third * ROW_TILE, ROW_TILE), :] = gated.astype(jnp.float32)
        if third == tiles - 1:
            halo_send[block] = gated[ROW_TILE - HALO :]

            @pl.when(s < n_sp - 1)
            def _():
                halo_copy(level, block).start()

    def gating(level, block):
        for third in order:
            gate(level, block, third)

    upper_half = z // (nz // 2)
    guest_chip = 1 - upper_half
    host = jnp.logical_and(middle, chip == guest_chip)
    feeder = jnp.logical_and(middle, chip != guest_chip)
    lender = jnp.logical_and(outer, chip == guest_chip)
    keeper = jnp.logical_and(outer, chip != guest_chip)

    def guest_copy(kind, third):
        span = pl.ds(third * ROW_TILE, ROW_TILE)
        inward = s + 2 - 4 * upper_half
        outward = s - 2 + 4 * upper_half
        source, target, place, mate = (
            (scaled.at[span, :], guest.at[span, :], inward, t),
            (guest_part.at[1, third], guest_core.at[third], s, core_mate),
            (guest_out.at[third], guest_in.at[third], s, chip_mate),
            (guest_gated.at[third], lent.at[third], outward, t),
            (guest_sum, guest_sums, inward, t),
        )[kind]
        return pltpu.make_async_remote_copy(
            src_ref=source,
            dst_ref=target,
            send_sem=g_send.at[kind * tiles + third],
            recv_sem=g_recv.at[kind * tiles + third],
            device_id=(place, mate),
            device_id_type=MESH,
        )

    def guest_start():
        guest_copy(4, 0).start()
        for third in order[:-1]:
            guest_copy(0, third).start()
        guest_copy(0, order[-1]).start()
        own_column(1)

    def guest_left():
        guest_copy(4, 0).wait_send()
        for third in order:
            guest_copy(0, third).wait_send()

    def guest_scale():
        guest_copy(4, 0).wait_recv()
        guest_scales[...] = lax.rsqrt(guest_sums[...] / D + row_floor).T

    def guest_products(third):
        guest_copy(0, third).wait_recv()
        span = pl.ds(third * ROW_TILE, ROW_TILE)

        for which in (1, 0):
            owner = (guest_chip * 2 + (core if which == 0 else 1 - core)) * blocks

            @pl.loop(0, blocks)
            def _(block, which=which, owner=owner):
                guest_part[which, third, block] = jnp.dot(
                    guest[span, :], w_in[0, owner + block], preferred_element_type=jnp.float32
                ).astype(jnp.bfloat16)

            if which == 1:
                guest_copy(1, third).start()

    def guest_pass(third):
        guest_copy(1, third).wait_recv()
        guest_out[third] = (
            guest_part[0, third].astype(jnp.float32) + guest_core[third].astype(jnp.float32)
        ).astype(jnp.bfloat16)
        guest_copy(2, third).start()

    def guest_gate(third):
        guest_copy(1, third).wait_recv()
        guest_copy(2, third).wait_recv()
        span = pl.ds(third * ROW_TILE, ROW_TILE)
        for block in range(blocks):
            total = (
                guest_part[0, third, block].astype(jnp.float32)
                + guest_core[third, block].astype(jnp.float32)
                + guest_in[third, block].astype(jnp.float32)
            ) * guest_scales[span, 0:1]
            guest_gated[third, block] = (
                total[:, :piece] * jax.nn.sigmoid(total[:, piece:])
            ).astype(jnp.bfloat16)
        guest_copy(3, third).start()

    def lend(third):
        guest_copy(3, third).wait_recv()
        for block in range(blocks):
            extended[block, pl.ds(HALO + third * ROW_TILE, ROW_TILE), :] = lent[
                third, block
            ].astype(jnp.float32)
            if third == tiles - 1:
                halo_send[block] = lent[third, block, ROW_TILE - HALO :, :]

                @pl.when(s < n_sp - 1)
                def _(block=block):
                    halo_copy(0, block).start()

    def guest_settle():
        for third in order:
            apart(middle, (guest_sent, 1, third))
            apart(feeder, (guest_sent, 2, third))
            apart(host, (guest_sent, 3, third))

    def guest_sent(kind, third):
        guest_copy(kind, third).wait_send()

    per_part = ROW_TILE // CONV_TILE

    def convolve(level, block, third):
        bias = taps[level, block, pl.ds(width, 1), :]
        weights = taps[level, block]

        @pl.loop(third * per_part, (third + 1) * per_part)
        def _(tile):
            start = pl.multiple_of(tile * CONV_TILE, CONV_TILE)
            window = extended[block, pl.ds(start, CONV_TILE + HALO), :]
            total = jnp.zeros((CONV_TILE, piece), jnp.float32) + bias
            for offset in range(width):
                low = HALO - reach + offset
                total = total + weights[offset : offset + 1, :] * window[low : low + CONV_TILE]
            filtered[block, pl.ds(start, CONV_TILE), :] = total

    def first_rows(level, block):
        @pl.when(s > 0)
        def _():
            halo_copy(level, block).wait_recv()
            extended[block, pl.ds(0, HALO), :] = halo_recv[level, block].astype(jnp.float32)

        @pl.when(s == 0)
        def _():
            extended[block, pl.ds(0, HALO), :] = jnp.zeros((HALO, piece), jnp.float32)

    def normalise(level, third):
        ggain = ggain_ref[pl.ds(level, 1), :].astype(jnp.float32)
        gshift = gshift_ref[pl.ds(level, 1), :].astype(jnp.float32)

        @pl.loop(third * per_part, (third + 1) * per_part)
        def _(tile):
            span = pl.ds(pl.multiple_of(tile * CONV_TILE, CONV_TILE), CONV_TILE)
            pieces = [filtered[block, span, :] for block in range(blocks)]
            mean = sum(jnp.sum(value, axis=1, keepdims=True) for value in pieces) / channels
            pieces = [value - mean for value in pieces]
            var = sum(jnp.sum(value * value, axis=1, keepdims=True) for value in pieces) / channels
            factor = lax.rsqrt(var + group_floor)
            for block in range(blocks):
                lanes = slice(block * piece, (block + 1) * piece)
                normed = pieces[block] * factor * ggain[:, lanes] + gshift[:, lanes]
                mixed[level, t, span, lanes] = (normed * jax.nn.sigmoid(normed)).astype(
                    jnp.bfloat16
                )

        mixed_copy(level, 1, third).start()
        mixed_copy(level, 0, third).start()

    def relay(level, third):
        mixed_copy(level, 1, third).wait_recv()
        mixed_copy(level, 2, third).start()

    def projecting(level, third):
        mixed_copy(level, 0, third).wait_recv()
        mixed_copy(level, 2, third).wait_recv()
        span = pl.ds(third * ROW_TILE, ROW_TILE)
        total = held[span, :].astype(jnp.float32)
        for owner in range(n_tp):
            total = total + jnp.dot(
                mixed[level, owner, span, :],
                w_out[level, pl.ds(owner * channels, channels), :],
                preferred_element_type=jnp.float32,
            )
        held[span, :] = total.astype(jnp.bfloat16)
        if level + 1 < layers:
            prepare(level + 1, third)
        else:
            result_copy(third).start()

    def result_copy(third):
        span = pl.ds(third * ROW_TILE, ROW_TILE)
        return pltpu.make_async_copy(held.at[span, :], out_ref.at[span, :], result_sem.at[third])

    def settle(level):
        for target_chip in range(2):
            used = middle if level == 0 else z >= 0

            @pl.when(jnp.logical_or(used, target_chip != guest_chip))
            def _(target_chip=target_chip):
                for block in range(blocks):
                    for third in order:
                        core_copy(level, target_chip, block, third).wait_send()

        passed = jnp.logical_or(middle, lender) if level == 0 else z >= 0

        @pl.when(passed)
        def _():
            for block in range(blocks):
                for third in order:
                    chip_copy(level, block, third).wait_send()

        for slot in range(3):
            for third in order:
                mixed_copy(level, slot, third).wait_send()

        @pl.when(s < n_sp - 1)
        def _():
            for block in range(blocks):
                halo_copy(level, block).wait_send()

    own_rows(0)
    own_column(0)
    for copy in loads[2:]:
        copy.wait()
    for level in range(layers):
        for block in range(blocks):
            lanes = slice(block * piece, (block + 1) * piece)
            taps[level, block, 0:width, :] = taps_ref[:, level, lanes].astype(jnp.float32)
            taps[level, block, width : width + 1, :] = bias_ref[level : level + 1, lanes].astype(
                jnp.float32
            )
    taken.wait()
    for tile in range(tiles):
        prepare(0, tile)
    for copy in square_copies(0):
        copy.start()
    row_scales(0)
    goals = [target_of(turn_index) for turn_index in range(n_tp)]

    def late(third):
        for block in (y, 1 - y):
            convolve(0, block, third)
        normalise(0, third)

    def end_start():
        turn(0)
        guest_start()
        contribute(0, goals[0], 0)
        hop(0, 1)
        own_rows(1)
        contribute(0, goals[1], 0)
        contribute(0, goals[0], 1)
        pass_on(0, goals[0], 0)
        pass_on(0, goals[1], 0)
        contribute(0, goals[1], 1)
        pass_on(0, goals[0], 1)
        pass_on(0, goals[1], 1)
        turn(1)
        apart(jnp.logical_or(z > 0, y == 0), (own_column, 2))
        hop(1, 1)
        own_rows(2)
        apart(
            keeper,
            (gating, 0, y),
            (gating, 0, 1 - y),
        )
        hop(1, 2)
        hop(2, 1)
        apart(
            keeper,
            *((convolve, 0, y, third) for third in order[:-1]),
            *(
                step
                for third in order[:-1]
                for step in ((convolve, 0, 1 - y, third), (normalise, 0, third))
            ),
        )
        apart(lender, (lend, order[0]))
        apart(jnp.logical_and(z == 0, y == 1), (own_column, 2))
        turn(2)
        apart(lender, (lend, order[1]), (late, order[0]))
        hop(1, 3, (0,))
        hop(2, 2)
        own_column(3)
        apart(lender, (lend, order[2]), (late, order[1]))
        hop(1, 3, (1,))

    def middle_start():
        for phase in range(1, len(phases)):
            own_column(phase, True)
        contribute(0, goals[0], 0)
        hop(0, 1)
        contribute(0, goals[1], 0)
        contribute(0, goals[2], 0)
        contribute(0, goals[0], 1)
        pass_on(0, goals[0], 0)
        pass_on(0, goals[1], 0)
        pass_on(0, goals[2], 0)
        side(0, 1)
        hop(0, 2)
        own_rows(1)
        own_column(1, False)
        contribute(0, goals[3], 0)
        pass_on(0, goals[0], 1)
        contribute(0, goals[1], 1)
        pass_on(0, goals[3], 0)
        pass_on(0, goals[1], 1)
        contribute(0, goals[2], 1)
        side(0, 2)
        pass_on(0, goals[2], 1)
        contribute(0, goals[3], 1)
        own_column(2, False)
        guest_scale()
        guest_products(order[0])
        hop(1, 1, (0, 1), False)
        apart(feeder, (guest_pass, order[0]))
        pass_on(0, goals[3], 1)
        guest_products(order[1])
        gating(0, y)
        for third in order[:-1]:
            convolve(0, y, third)
        hop(2, 1, (0,), False)
        apart(feeder, (guest_pass, order[1]))
        hop(2, 1, (1,), False)
        own_column(3, False)
        apart(host, (guest_gate, order[0]))
        gating(0, 1 - y)
        guest_products(order[2])
        apart(feeder, (guest_pass, order[2]))
        hop(1, 1, (0,), True)
        for third in order[:-1]:
            convolve(0, 1 - y, third)
            normalise(0, third)
        apart(host, (guest_gate, order[1]))
        hop(1, 1, (1,), True)
        hop(1, 2, (0,))
        own_rows(2)
        side(1, 1)
        hop(1, 2, (1,))
        apart(host, (guest_gate, order[2]))
        side(1, 2)
        hop(2, 1, (0,), True)
        hop(3, 1, (0, 1), False)

    apart(outer, (end_start,))
    apart(middle, (middle_start,))
    for level in range(layers):
        first, second = 2 * level, 2 * level + 1
        last = level == layers - 1
        targets = [target_of(turn_index) for turn_index in range(n_tp)]
        if level > 0:
            apart(outer, (hop, first, 3, (0,)), (own_rows, second), (hop, second, 1))
            contribute(level, targets[0], 0)
            contribute(level, targets[1], 0)
            apart(middle, (hop, second, 1, (0, 1), True))
            contribute(level, targets[0], 1)
            pass_on(level, targets[0], 0)
            contribute(level, targets[2], 0)
            pass_on(level, targets[1], 0)
            pass_on(level, targets[0], 1)
            contribute(level, targets[1], 1)
            pass_on(level, targets[2], 0)
            apart(middle, (side, first, nz - 2))
            contribute(level, targets[2], 1)
            pass_on(level, targets[1], 1)
            pass_on(level, targets[2], 1)
            apart(outer, (turn, second), (hop, first, 3, (1,)))
            contribute(level, targets[3], 0)
            apart(outer, (hop, second, 2))
            apart(middle, (own_rows, second))
            pass_on(level, targets[3], 0)
            apart(outer, (side, first, nz - 1))
            contribute(level, targets[3], 1)
            pass_on(level, targets[3], 1)
            apart(middle, (hop, second, 2))
            row_scales(level)
            gating(level, y)
            for third in order[:-1]:
                convolve(level, y, third)
            gate(level, 1 - y, order[0])
            for index in range(1, tiles):
                gate(level, 1 - y, order[index])
                convolve(level, 1 - y, order[index - 1])
                normalise(level, order[index - 1])
                if index == 1:
                    apart(outer, (hop, second, 3, (0,)))
            apart(middle, (side, second, 1), (side, second, 2))
        for block in (y, 1 - y):
            first_rows(level, block)
            convolve(level, block, order[-1])
        normalise(level, order[-1])
        relay(level, order[0])
        if level > 0:
            apart(outer, (hop, second, 3, (1,)), (side, second, nz - 1))
        else:
            apart(outer, (guest_left,), (side, second, nz - 1))
        for source in range(nz):
            crossed(second, source)
        if not last:
            apart(middle, (hop, first + 2, 1, (1,), True))
        for index in range(1, tiles):
            relay(level, order[index])
            projecting(level, order[index - 1])
            if not last and index == 1:
                apart(middle, (hop, first + 2, 2, (0,)))
            if not last and index == 2:
                apart(middle, (side, first + 2, 1))
        projecting(level, order[-1])
        if not last:
            for copy in square_copies(level + 1):
                copy.start()
            apart(middle, (hop, first + 2, 2, (1,)))
        settle(level)
    guest_settle()
    for phase in range(len(phases)):
        sent(phase)
    for third in order:
        result_copy(third).wait()


def fused(n_sp, n_tp, *arrays):
    hidden_in, norm_gain, value_proj = arrays[:3]
    rows, feats = hidden_in.shape
    layers = norm_gain.shape[0]
    piece = value_proj.shape[2]
    blocks = n_sp // n_tp
    channels = blocks * piece
    kinds = 4
    tiles = rows // ROW_TILE
    vmem = pl.BlockSpec(memory_space=pltpu.VMEM)
    hbm = pl.BlockSpec(memory_space=pltpu.HBM)
    low, wide = jnp.bfloat16, jnp.float32
    slots = layers * blocks + 3 * (blocks + 1) * (rows // ROW_TILE)
    arrays = arrays[:4] + (arrays[4].transpose(1, 0, 2),) + arrays[5:]
    return pl.pallas_call(
        lambda *refs: fused_kernel(n_sp, n_tp, *refs),
        out_shape=jax.ShapeDtypeStruct((rows, feats), low),
        in_specs=[hbm, vmem, hbm, hbm, vmem, vmem, vmem, vmem, hbm],
        out_specs=hbm,
        scratch_shapes=[
            pltpu.VMEM((rows, feats), low),
            pltpu.VMEM((layers, n_sp, feats, 2 * piece), low),
            pltpu.VMEM((layers, n_sp * piece, feats), low),
            pltpu.VMEM((rows, feats), low),
            pltpu.VMEM((n_tp, blocks, rows, 2 * piece), low),
            pltpu.VMEM((layers, 2, blocks, rows, 2 * piece), low),
            pltpu.VMEM((blocks, rows, 2 * piece), low),
            pltpu.VMEM((layers, blocks, rows, 2 * piece), low),
            pltpu.VMEM((layers, blocks, WIDTH + 1, piece), wide),
            pltpu.VMEM((blocks, HALO + rows, piece), wide),
            pltpu.VMEM((blocks, HALO, piece), low),
            pltpu.VMEM((layers, blocks, HALO, piece), low),
            pltpu.VMEM((blocks, rows, piece), wide),
            pltpu.VMEM((layers, n_tp, rows, channels), low),
            pltpu.VMEM((layers, n_tp, 8, rows), wide),
            pltpu.VMEM((rows, 8), wide),
            pltpu.VMEM((rows, feats), low),
            pltpu.VMEM((2, tiles, blocks, ROW_TILE, 2 * piece), low),
            pltpu.VMEM((tiles, blocks, ROW_TILE, 2 * piece), low),
            pltpu.VMEM((tiles, blocks, ROW_TILE, 2 * piece), low),
            pltpu.VMEM((tiles, blocks, ROW_TILE, 2 * piece), low),
            pltpu.VMEM((tiles, blocks, ROW_TILE, piece), low),
            pltpu.VMEM((tiles, blocks, ROW_TILE, piece), low),
            pltpu.VMEM((8, rows), wide),
            pltpu.VMEM((8, rows), wide),
            pltpu.VMEM((rows, 8), wide),
            pltpu.SemaphoreType.DMA((layers, kinds)),
            pltpu.SemaphoreType.DMA((rows // ROW_TILE,)),
            pltpu.SemaphoreType.DMA((layers * 2, 2 * n_sp + 4)),
            pltpu.SemaphoreType.DMA((layers * 2, 2, n_sp)),
            pltpu.SemaphoreType.DMA((slots,)),
            pltpu.SemaphoreType.DMA((slots,)),
            pltpu.SemaphoreType.DMA((3,)),
            pltpu.SemaphoreType.DMA((3,)),
            pltpu.SemaphoreType.DMA((4 * tiles + 1,)),
            pltpu.SemaphoreType.DMA((4 * tiles + 1,)),
        ],
        compiler_params=pltpu.CompilerParams(
            collective_id=0, has_side_effects=True, vmem_limit_bytes=VMEM_BYTES
        ),
    )(*arrays)


def solution(mesh):
    n_sp, n_tp = mesh.shape["sp"], mesh.shape["tp"]
    piece = C // n_sp
    small = n_tp == 4 and GROUPS == n_tp and n_sp == 8 and piece % 128 == 0

    def local(*arrays):
        if small and arrays[0].shape[0] % ROW_TILE == 0:
            return fused(n_sp, n_tp, *arrays)
        return on_device(*arrays)

    return jax.shard_map(
        local,
        mesh=mesh,
        in_specs=(
            P("sp", "tp"),
            P(None, "tp"),
            P(None, "tp", "sp"),
            P(None, "tp", "sp"),
            P(None, None, "tp"),
            P(None, "tp"),
            P(None, "tp"),
            P(None, "tp"),
            P(None, "sp", "tp"),
        ),
        out_specs=P("sp", "tp"),
        check_vma=False,
    )
```

```python
import jax
import jax.numpy as jnp
from jax import lax
from jax.experimental import pallas as pl
from jax.experimental.pallas import tpu as pltpu
from jax.sharding import PartitionSpec as P

D = 4096
C = 1024
GROUPS = 4
WIDTH = 31


row_floor = 1e-06
group_floor = 1e-05


def passed_along(value, axis, steps):
    count = lax.axis_size(axis)
    initial, last = (max(0, -steps), min(count, count - steps))
    return lax.ppermute(value, axis, [(source, source + steps) for source in range(initial, last)])


def rms_normed(residual_rows, gain_part):
    wide_rows = residual_rows.astype(jnp.float32)
    squares = lax.psum(jnp.sum(wide_rows * wide_rows, axis=1), "tp")
    scale_rows = lax.rsqrt(squares / D + row_floor)
    return (wide_rows * scale_rows[:, None] * gain_part.astype(jnp.float32)[None, :]).astype(
        jnp.bfloat16
    )


def gated_input(normed_rows, w_value, w_gate):
    numbers = (((0,), (1,)), ((), ()))
    value_part = lax.dot_general(w_value, normed_rows, numbers, preferred_element_type=jnp.float32)
    gate_part = lax.dot_general(w_gate, normed_rows, numbers, preferred_element_type=jnp.float32)
    summed = lax.psum_scatter(
        jnp.stack([value_part, gate_part], axis=1).astype(jnp.bfloat16),
        "tp",
        scatter_dimension=0,
        tiled=True,
    ).astype(jnp.float32)
    return (summed[:, 0] * jax.nn.sigmoid(summed[:, 1])).astype(jnp.bfloat16)


def depthwise(extended, taps_part, bias_part, out_len):
    widened = extended.astype(jnp.float32)
    taps = taps_part.astype(jnp.float32)
    filtered = (
        jnp.zeros((extended.shape[0], out_len), jnp.float32)
        + bias_part.astype(jnp.float32)[:, None]
    )
    for offset in range(WIDTH):
        filtered = filtered + taps[offset][:, None] * widened[:, offset : offset + out_len]
    return filtered


def group_normed(filtered, gain_part, shift_part, group_size):
    channels, out_len = filtered.shape
    grouped = filtered.reshape(channels // group_size, group_size, out_len)
    group_mean = jnp.mean(grouped, axis=1, keepdims=True)
    centered = grouped - group_mean
    group_var = jnp.mean(centered * centered, axis=1, keepdims=True)
    scaled = (centered * lax.rsqrt(group_var + group_floor)).reshape(channels, out_len)
    scaled = (
        scaled * gain_part.astype(jnp.float32)[:, None] + shift_part.astype(jnp.float32)[:, None]
    )
    return jax.nn.silu(scaled).astype(jnp.bfloat16)


def project_out(mixed, w_out):
    return lax.dot_general(
        lax.all_gather(mixed, "tp", axis=0, tiled=True),
        w_out,
        (((0,), (0,)), ((), ())),
        preferred_element_type=jnp.float32,
    )


def on_device(
    hidden_in,
    norm_gain,
    value_proj,
    gate_proj,
    conv_taps,
    conv_bias,
    group_gain,
    group_shift,
    out_proj,
):
    tok_rows = hidden_in.shape[0]
    layers = norm_gain.shape[0]
    reach_back = WIDTH - 1
    group_size = C // GROUPS
    all_value, all_gate, all_out = (
        lax.all_gather(value_proj, "sp", axis=2, tiled=True),
        lax.all_gather(gate_proj, "sp", axis=2, tiled=True),
        lax.all_gather(out_proj, "sp", axis=1, tiled=True),
    )
    residual_rows = hidden_in
    for level in range(layers):
        w_value, w_gate, w_out = (all_value[level], all_gate[level], all_out[level])
        normed_rows = rms_normed(residual_rows, norm_gain[level])
        gated = gated_input(normed_rows, w_value, w_gate)
        before = passed_along(gated[:, tok_rows - reach_back :], "sp", 1)
        extended = jnp.concatenate([before, gated], axis=1)
        out_len = extended.shape[1] - reach_back
        filtered = depthwise(extended, conv_taps[level], conv_bias[level], out_len)
        mixed = group_normed(filtered, group_gain[level], group_shift[level], group_size)
        update = project_out(mixed, w_out)
        kept_rows = residual_rows
        residual_rows = (kept_rows.astype(jnp.float32) + update).astype(jnp.bfloat16)
    return residual_rows


MESH = pl.DeviceIdType.MESH
HALO = 32
ROW_TILE = 256
CONV_TILE = 64
VMEM_BYTES = 62 * 1024 * 1024


def fused_kernel(
    n_sp,
    n_tp,
    hidden_ref,
    norm_ref,
    value_ref,
    gate_ref,
    taps_ref,
    bias_ref,
    ggain_ref,
    gshift_ref,
    out_proj_ref,
    out_ref,
    held,
    w_in,
    w_out,
    scaled,
    part,
    from_core,
    to_chip,
    from_chip,
    taps,
    extended,
    halo_send,
    halo_recv,
    filtered,
    mixed,
    squares,
    scales,
    guest,
    guest_part,
    guest_core,
    guest_out,
    guest_in,
    guest_gated,
    lent,
    guest_sum,
    guest_sums,
    guest_scales,
    load_sem,
    result_sem,
    w_send,
    w_recv,
    t_send,
    t_recv,
    s_send,
    s_recv,
    g_send,
    g_recv,
):
    width, layers = taps_ref.shape[0], taps_ref.shape[1]
    rows, feats = hidden_ref.shape
    piece = value_ref.shape[2]
    blocks = n_sp // n_tp
    channels = blocks * piece
    reach = width - 1
    nz = n_sp // 2
    s = lax.axis_index("sp")
    t = lax.axis_index("tp")
    z, y = s // 2, s % 2
    chip, core = t // 2, t % 2
    core_mate = chip * 2 + (1 - core)
    chip_mate = (1 - chip) * 2 + core
    far_mate = (1 - chip) * 2 + (1 - core)
    across = z * 2 + 1 - y

    taken = pltpu.make_async_copy(hidden_ref, held, load_sem.at[0, 3])
    loads = []
    for level in range(layers):
        for kind, (source, target) in enumerate(
            (
                (value_ref.at[level], w_in.at[level, s, :, pl.ds(0, piece)]),
                (gate_ref.at[level], w_in.at[level, s, :, pl.ds(piece, piece)]),
                (
                    out_proj_ref.at[level],
                    w_out.at[level, pl.ds(pl.multiple_of(s * piece, piece), piece), :],
                ),
            )
        ):
            copy = pltpu.make_async_copy(source, target, load_sem.at[level, kind])
            copy.start()
            loads.append(copy)

    taken.start()
    barrier = pltpu.get_barrier_semaphore()

    def greet(sp_index, tp_index):
        pl.semaphore_signal(barrier, inc=1, device_id=(sp_index, tp_index), device_id_type=MESH)

    up, down = z < nz - 1, z > 0
    corner_up = jnp.logical_and(up, y == 1)
    corner_down = jnp.logical_and(down, y == 0)
    for mate in (core_mate, chip_mate, far_mate):
        greet(s, mate)
    greet(across, t)
    for condition, target in (
        (up, s + 2),
        (down, s - 2),
        (corner_up, s + 1),
        (corner_down, s - 1),
    ):

        @pl.when(condition)
        def _(target=target):
            greet(target, t)

    mates = 4
    for condition in (up, down, corner_up, corner_down):
        mates = mates + condition.astype(jnp.int32)
    pl.semaphore_wait(barrier, mates)

    for copy in loads[:2]:
        copy.wait()

    phases = []
    for level in range(layers):
        phases += [("in", level), ("out", level)]

    def chunk(phase, owner, lot):
        kind, level = phases[phase]
        if kind == "in":
            size = feats // 2
            return w_in.at[level, owner, pl.ds(lot * size, size), :]
        size = piece // 2
        return w_out.at[
            level, pl.ds(pl.multiple_of(owner * piece + lot * size, size), size), :
        ]

    def place_of(owner, way, lot):
        source, column = owner // 2, owner % 2
        if way == 2:
            return 2 * source + lot
        return 2 * nz + (2 * (source + way) + lot) * (1 - (column + y) % 2) + (
            2 * (nz + 1) + way
        ) * ((column + y) % 2)

    def weight_copy(phase, owner, way, lot):
        return pltpu.make_async_remote_copy(
            src_ref=chunk(phase, owner, lot),
            dst_ref=chunk(phase, owner, lot),
            send_sem=w_send.at[phase, place_of(owner, way, lot)],
            recv_sem=w_recv.at[phase, lot, owner],
            device_id=((s + 2, s - 2, across)[way], t),
            device_id_type=MESH,
        )

    def go(phase, owner, way, lot, finish):
        copy = weight_copy(phase, owner, way, lot)
        if finish:
            copy.wait_send()
        else:
            copy.start()

    def come(phase, owner, lot, finish):
        if not finish:
            weight_copy(phase, owner, 2, lot).wait_recv()

    outer = jnp.logical_or(z == 0, z == nz - 1)
    middle = jnp.logical_and(z > 0, z < nz - 1)

    def own_rows(phase, finish=False):
        for lot in (1, 0):
            go(phase, s, 2, lot, finish)

    def own_column(phase, ends=None, finish=False):
        to_end = (z == nz - 2, z == 1)
        to_middle = (z < nz - 2, z > 1)
        conditions = (up, down) if ends is None else to_end if ends else to_middle
        for lot in (0, 1):
            for way, condition in enumerate(conditions):

                @pl.when(condition)
                def _(way=way, lot=lot):
                    go(phase, s, way, lot, finish)

    def turn(phase, finish=False):
        for way, place in enumerate((0, nz - 1)):

            @pl.when(z == place)
            def _(way=way):
                come(phase, across, 1, finish)
                go(phase, across, way, 1, finish)

    def hop(phase, steps, lots=(0, 1), ends=None, finish=False):
        for lot in lots:
            for way, sign in enumerate((-1, 1)):
                source = z + sign * steps
                inside = source >= 0 if way == 0 else source < nz
                inner = source > 0 if way == 0 else source < nz - 1
                onward = up if way == 0 else down
                if phase == 0:
                    onward = z < nz - 2 if way == 0 else z > 1
                    if steps > 1:
                        inside = jnp.logical_and(inside, middle)
                if ends is not None:
                    place = 0 if way == 0 else nz - 1
                    inside = source == place if ends else jnp.logical_and(inside, inner)

                @pl.when(inside)
                def _(way=way, lot=lot, source=source, inner=inner, onward=onward):
                    owner = source * 2 + y
                    come(phase, owner, lot, finish)

                    @pl.when(onward)
                    def _():
                        go(phase, owner, way, lot, finish)

                    if lot == 0:
                        go(phase, owner, 2, lot, finish)
                    else:

                        @pl.when(inner)
                        def _():
                            go(phase, owner, 2, lot, finish)

    def side(phase, steps, finish=False):
        if phase == 0 and steps == nz - 1:
            return
        for way, place in enumerate((0, nz - 1)):
            source = z - steps if way == 0 else z + steps
            onward = up if way == 0 else down
            if phase == 0:
                onward = z < nz - 2 if way == 0 else z > 1

            @pl.when(source == place)
            def _(way=way, place=place, onward=onward):
                owner = place * 2 + 1 - y
                come(phase, owner, 1, finish)

                @pl.when(onward)
                def _():
                    go(phase, owner, way, 1, finish)

    def apart(condition, *steps):
        @pl.when(condition)
        def _():
            for function, *arguments in steps:
                function(*arguments)

    def crossed(phase, source):
        owner = source * 2 + 1 - y
        come(phase, owner, 0, False)

        @pl.when(jnp.logical_and(source > 0, source < nz - 1))
        def _():
            come(phase, owner, 1, False)

    def sent(phase):
        own_rows(phase, True)
        own_column(phase, finish=True)
        turn(phase, True)
        for steps in range(1, nz):
            hop(phase, steps, finish=True)
            side(phase, steps, finish=True)

    def tp_copy(level, slot, source, target, mate, sp_index=None):
        return pltpu.make_async_remote_copy(
            src_ref=source,
            dst_ref=target,
            send_sem=t_send.at[slot],
            recv_sem=t_recv.at[slot],
            device_id=(s if sp_index is None else sp_index, mate),
            device_id_type=MESH,
        )

    tiles = rows // ROW_TILE
    order = tuple(reversed(range(tiles)))

    def prepare(level, tile):
        gain = norm_ref[pl.ds(level, 1), :].astype(jnp.float32)
        ones = jnp.ones((8, feats), jnp.bfloat16)
        numbers = (((1,), (1,)), ((), ()))
        span = pl.ds(tile * ROW_TILE, ROW_TILE)
        wide = held[span, :].astype(jnp.float32)
        scaled[span, :] = (wide * gain).astype(jnp.bfloat16)
        square = wide * wide
        high = square.astype(jnp.bfloat16)
        low = (square - high.astype(jnp.float32)).astype(jnp.bfloat16)
        total = lax.dot_general(ones, high, numbers, preferred_element_type=jnp.float32)
        total = total + lax.dot_general(ones, low, numbers, preferred_element_type=jnp.float32)
        squares[level, t, :, span] = total

    def square_copies(level):
        return [
            pltpu.make_async_remote_copy(
                src_ref=squares.at[level, t],
                dst_ref=squares.at[level, t],
                send_sem=s_send.at[slot],
                recv_sem=s_recv.at[slot],
                device_id=(s, mate),
                device_id_type=MESH,
            )
            for slot, mate in enumerate((core_mate, chip_mate, far_mate))
        ]

    def row_scales(level):
        for copy in square_copies(level):
            copy.wait_send()
            copy.wait_recv()
        total = squares[level, 0]
        for index in range(1, n_tp):
            total = total + squares[level, index]
        scales[...] = lax.rsqrt(total / D + row_floor).T
        if level == 0:
            guest_sum[...] = total

    def rows_of(third):
        return pl.ds(pl.multiple_of(third * ROW_TILE, ROW_TILE), ROW_TILE)

    def core_copy(level, target_chip, block, third):
        owner = target_chip * 2 + 1 - core
        return tp_copy(
            level,
            (target_chip * blocks + block) * tiles + third,
            part.at[owner, block, rows_of(third), :],
            from_core.at[level, target_chip, block, rows_of(third), :],
            core_mate,
        )

    base = 3 * blocks * tiles - blocks

    def chip_copy(level, block, third):
        return tp_copy(
            level,
            (2 * blocks + block) * tiles + third,
            to_chip.at[block, rows_of(third), :],
            from_chip.at[level, block, rows_of(third), :],
            chip_mate,
        )

    def halo_copy(level, block):
        return tp_copy(
            level,
            base + (1 + level) * blocks + block,
            halo_send.at[block],
            halo_recv.at[level, block],
            t,
            s + 1,
        )

    def mixed_copy(level, slot, third):
        owner = (t, t, chip_mate)[slot]
        mate = (core_mate, chip_mate, core_mate)[slot]
        block = mixed.at[level, owner, pl.ds(third * ROW_TILE, ROW_TILE), :]
        return tp_copy(level, base + (1 + layers) * blocks + slot * tiles + third, block, block, mate)

    def target_of(turn_index):
        upper = z // (nz // 2)
        near = z + upper * (nz - 1 - 2 * z)
        pick = (near, 1 - near)[turn_index] if turn_index < 2 else turn_index
        return pick + upper * (nz - 1 - 2 * pick)

    def products(level, target, block):
        @pl.loop(0, tiles)
        def _(step):
            third = tiles - 1 - step
            span = rows_of(third)
            part[target, block, span, :] = jnp.dot(
                scaled[span, :],
                w_in[level, target * blocks + block],
                preferred_element_type=jnp.float32,
            ).astype(jnp.bfloat16)

            @pl.when(target % 2 != core)
            def _():
                core_copy(level, target // 2, block, third).start()

    def contribute(level, target, turned):
        block = 1 - y if turned else y
        if turned:
            crossed(2 * level, target)
        products(level, target, block)

    def pass_on(level, target, turned):
        block = 1 - y if turned else y

        @pl.when(target == chip_mate)
        def _():
            @pl.loop(0, tiles)
            def _(step):
                third = tiles - 1 - step
                span = rows_of(third)
                core_copy(level, 1 - chip, block, third).wait_recv()
                to_chip[block, span, :] = (
                    part[chip_mate, block, span, :].astype(jnp.float32)
                    + from_core[level, 1 - chip, block, span, :].astype(jnp.float32)
                ).astype(jnp.bfloat16)
                chip_copy(level, block, third).start()

    def gate(level, block, third):
        core_copy(level, chip, block, third).wait_recv()
        chip_copy(level, block, third).wait_recv()
        span = rows_of(third)
        total = (
            part[t, block, span, :].astype(jnp.float32)
            + from_core[level, chip, block, span, :].astype(jnp.float32)
            + from_chip[level, block, span, :].astype(jnp.float32)
        ) * scales[span, 0:1]
        gated = (total[:, :piece] * jax.nn.sigmoid(total[:, piece:])).astype(jnp.bfloat16)
        extended[block, pl.ds(HALO + third * ROW_TILE, ROW_TILE), :] = gated.astype(jnp.float32)
        if third == tiles - 1:
            halo_send[block] = gated[ROW_TILE - HALO :]

            @pl.when(s < n_sp - 1)
            def _():
                halo_copy(level, block).start()

    def gating(level, block):
        for third in order:
            gate(level, block, third)

    upper_half = z // (nz // 2)
    guest_chip = 1 - upper_half
    host = jnp.logical_and(middle, chip == guest_chip)
    feeder = jnp.logical_and(middle, chip != guest_chip)
    lender = jnp.logical_and(outer, chip == guest_chip)
    keeper = jnp.logical_and(outer, chip != guest_chip)

    def guest_copy(kind, third):
        span = pl.ds(third * ROW_TILE, ROW_TILE)
        inward = s + 2 - 4 * upper_half
        outward = s - 2 + 4 * upper_half
        source, target, place, mate = (
            (scaled.at[span, :], guest.at[span, :], inward, t),
            (guest_part.at[1, third], guest_core.at[third], s, core_mate),
            (guest_out.at[third], guest_in.at[third], s, chip_mate),
            (guest_gated.at[third], lent.at[third], outward, t),
            (guest_sum, guest_sums, inward, t),
        )[kind]
        return pltpu.make_async_remote_copy(
            src_ref=source,
            dst_ref=target,
            send_sem=g_send.at[kind * tiles + third],
            recv_sem=g_recv.at[kind * tiles + third],
            device_id=(place, mate),
            device_id_type=MESH,
        )

    def guest_start():
        guest_copy(4, 0).start()
        for third in order[:-1]:
            guest_copy(0, third).start()
        guest_copy(0, order[-1]).start()
        own_column(1)

    def guest_left():
        guest_copy(4, 0).wait_send()
        for third in order:
            guest_copy(0, third).wait_send()

    def guest_scale():
        guest_copy(4, 0).wait_recv()
        guest_scales[...] = lax.rsqrt(guest_sums[...] / D + row_floor).T

    def guest_products(third):
        guest_copy(0, third).wait_recv()
        span = pl.ds(third * ROW_TILE, ROW_TILE)

        for which in (1, 0):
            owner = (guest_chip * 2 + (core if which == 0 else 1 - core)) * blocks

            @pl.loop(0, blocks)
            def _(block, which=which, owner=owner):
                guest_part[which, third, block] = jnp.dot(
                    guest[span, :], w_in[0, owner + block], preferred_element_type=jnp.float32
                ).astype(jnp.bfloat16)

            if which == 1:
                guest_copy(1, third).start()

    def guest_pass(third):
        guest_copy(1, third).wait_recv()
        guest_out[third] = (
            guest_part[0, third].astype(jnp.float32) + guest_core[third].astype(jnp.float32)
        ).astype(jnp.bfloat16)
        guest_copy(2, third).start()

    def guest_gate(third):
        guest_copy(1, third).wait_recv()
        guest_copy(2, third).wait_recv()
        span = pl.ds(third * ROW_TILE, ROW_TILE)
        for block in range(blocks):
            total = (
                guest_part[0, third, block].astype(jnp.float32)
                + guest_core[third, block].astype(jnp.float32)
                + guest_in[third, block].astype(jnp.float32)
            ) * guest_scales[span, 0:1]
            guest_gated[third, block] = (
                total[:, :piece] * jax.nn.sigmoid(total[:, piece:])
            ).astype(jnp.bfloat16)
        guest_copy(3, third).start()

    def lend(third):
        guest_copy(3, third).wait_recv()
        for block in range(blocks):
            extended[block, pl.ds(HALO + third * ROW_TILE, ROW_TILE), :] = lent[
                third, block
            ].astype(jnp.float32)
            if third == tiles - 1:
                halo_send[block] = lent[third, block, ROW_TILE - HALO :, :]

                @pl.when(s < n_sp - 1)
                def _(block=block):
                    halo_copy(0, block).start()

    def guest_settle():
        for third in order:
            apart(middle, (guest_sent, 1, third))
            apart(feeder, (guest_sent, 2, third))
            apart(host, (guest_sent, 3, third))

    def guest_sent(kind, third):
        guest_copy(kind, third).wait_send()

    per_part = ROW_TILE // CONV_TILE

    def convolve(level, block, third):
        bias = taps[level, block, pl.ds(width, 1), :]
        weights = taps[level, block]

        @pl.loop(third * per_part, (third + 1) * per_part)
        def _(tile):
            start = pl.multiple_of(tile * CONV_TILE, CONV_TILE)
            window = extended[block, pl.ds(start, CONV_TILE + HALO), :]
            total = jnp.zeros((CONV_TILE, piece), jnp.float32) + bias
            for offset in range(width):
                low = HALO - reach + offset
                total = total + weights[offset : offset + 1, :] * window[low : low + CONV_TILE]
            filtered[block, pl.ds(start, CONV_TILE), :] = total

    def first_rows(level, block):
        @pl.when(s > 0)
        def _():
            halo_copy(level, block).wait_recv()
            extended[block, pl.ds(0, HALO), :] = halo_recv[level, block].astype(jnp.float32)

        @pl.when(s == 0)
        def _():
            extended[block, pl.ds(0, HALO), :] = jnp.zeros((HALO, piece), jnp.float32)

    def normalise(level, third):
        ggain = ggain_ref[pl.ds(level, 1), :].astype(jnp.float32)
        gshift = gshift_ref[pl.ds(level, 1), :].astype(jnp.float32)

        @pl.loop(third * per_part, (third + 1) * per_part)
        def _(tile):
            span = pl.ds(pl.multiple_of(tile * CONV_TILE, CONV_TILE), CONV_TILE)
            pieces = [filtered[block, span, :] for block in range(blocks)]
            mean = sum(jnp.sum(value, axis=1, keepdims=True) for value in pieces) / channels
            pieces = [value - mean for value in pieces]
            var = sum(jnp.sum(value * value, axis=1, keepdims=True) for value in pieces) / channels
            factor = lax.rsqrt(var + group_floor)
            for block in range(blocks):
                lanes = slice(block * piece, (block + 1) * piece)
                normed = pieces[block] * factor * ggain[:, lanes] + gshift[:, lanes]
                mixed[level, t, span, lanes] = (normed * jax.nn.sigmoid(normed)).astype(
                    jnp.bfloat16
                )

        mixed_copy(level, 1, third).start()
        mixed_copy(level, 0, third).start()

    def relay(level, third):
        mixed_copy(level, 1, third).wait_recv()
        mixed_copy(level, 2, third).start()

    def projecting(level, third):
        mixed_copy(level, 0, third).wait_recv()
        mixed_copy(level, 2, third).wait_recv()
        span = pl.ds(third * ROW_TILE, ROW_TILE)
        total = held[span, :].astype(jnp.float32)
        for owner in range(n_tp):
            total = total + jnp.dot(
                mixed[level, owner, span, :],
                w_out[level, pl.ds(owner * channels, channels), :],
                preferred_element_type=jnp.float32,
            )
        held[span, :] = total.astype(jnp.bfloat16)
        if level + 1 < layers:
            prepare(level + 1, third)
        else:
            result_copy(third).start()

    def result_copy(third):
        span = pl.ds(third * ROW_TILE, ROW_TILE)
        return pltpu.make_async_copy(held.at[span, :], out_ref.at[span, :], result_sem.at[third])

    def settle(level):
        for target_chip in range(2):
            used = middle if level == 0 else z >= 0

            @pl.when(jnp.logical_or(used, target_chip != guest_chip))
            def _(target_chip=target_chip):
                for block in range(blocks):
                    for third in order:
                        core_copy(level, target_chip, block, third).wait_send()

        passed = jnp.logical_or(middle, lender) if level == 0 else z >= 0

        @pl.when(passed)
        def _():
            for block in range(blocks):
                for third in order:
                    chip_copy(level, block, third).wait_send()

        for slot in range(3):
            for third in order:
                mixed_copy(level, slot, third).wait_send()

        @pl.when(s < n_sp - 1)
        def _():
            for block in range(blocks):
                halo_copy(level, block).wait_send()

    own_rows(0)
    own_column(0)
    for copy in loads[2:]:
        copy.wait()
    for level in range(layers):
        for block in range(blocks):
            lanes = slice(block * piece, (block + 1) * piece)
            taps[level, block, 0:width, :] = taps_ref[:, level, lanes].astype(jnp.float32)
            taps[level, block, width : width + 1, :] = bias_ref[level : level + 1, lanes].astype(
                jnp.float32
            )
    taken.wait()
    for tile in range(tiles):
        prepare(0, tile)
    for copy in square_copies(0):
        copy.start()
    row_scales(0)
    goals = [target_of(turn_index) for turn_index in range(n_tp)]

    def late(third):
        for block in (y, 1 - y):
            convolve(0, block, third)
        normalise(0, third)

    def end_start():
        turn(0)
        guest_start()
        contribute(0, goals[0], 0)
        hop(0, 1)
        own_rows(1)
        contribute(0, goals[1], 0)
        contribute(0, goals[0], 1)
        pass_on(0, goals[0], 0)
        pass_on(0, goals[1], 0)
        contribute(0, goals[1], 1)
        pass_on(0, goals[0], 1)
        pass_on(0, goals[1], 1)
        turn(1)
        apart(jnp.logical_or(z > 0, y == 0), (own_column, 2))
        hop(1, 1)
        own_rows(2)
        apart(
            keeper,
            (gating, 0, y),
            (gating, 0, 1 - y),
        )
        hop(1, 2)
        hop(2, 1)
        apart(
            keeper,
            *((convolve, 0, y, third) for third in order[:-1]),
            *(
                step
                for third in order[:-1]
                for step in ((convolve, 0, 1 - y, third), (normalise, 0, third))
            ),
        )
        apart(lender, (lend, order[0]))
        apart(jnp.logical_and(z == 0, y == 1), (own_column, 2))
        turn(2)
        apart(lender, (lend, order[1]), (late, order[0]))
        hop(1, 3, (0,))
        hop(2, 2, (0,))
        own_column(3)
        own_rows(3)
        apart(lender, (lend, order[2]), (late, order[1]))
        hop(1, 3, (1,))

    def middle_start():
        for phase in range(1, len(phases)):
            own_column(phase, True)
        contribute(0, goals[0], 0)
        hop(0, 1)
        contribute(0, goals[1], 0)
        contribute(0, goals[2], 0)
        contribute(0, goals[0], 1)
        pass_on(0, goals[0], 0)
        pass_on(0, goals[1], 0)
        pass_on(0, goals[2], 0)
        side(0, 1)
        hop(0, 2)
        own_rows(1)
        own_column(1, False)
        contribute(0, goals[3], 0)
        pass_on(0, goals[0], 1)
        contribute(0, goals[1], 1)
        pass_on(0, goals[3], 0)
        pass_on(0, goals[1], 1)
        contribute(0, goals[2], 1)
        side(0, 2)
        pass_on(0, goals[2], 1)
        contribute(0, goals[3], 1)
        own_column(2, False)
        guest_scale()
        guest_products(order[0])
        hop(1, 1, (0, 1), False)
        apart(feeder, (guest_pass, order[0]))
        pass_on(0, goals[3], 1)
        guest_products(order[1])
        gating(0, y)
        for third in order[:-1]:
            convolve(0, y, third)
        hop(2, 1, (0,), False)
        apart(feeder, (guest_pass, order[1]))
        own_column(3, False)
        apart(host, (guest_gate, order[0]))
        gating(0, 1 - y)
        guest_products(order[2])
        apart(feeder, (guest_pass, order[2]))
        hop(1, 1, (0,), True)
        for third in order[:-1]:
            convolve(0, 1 - y, third)
            normalise(0, third)
        apart(host, (guest_gate, order[1]))
        hop(1, 1, (1,), True)
        hop(1, 2, (0,))
        own_rows(2)
        apart(host, (guest_gate, order[2]))
        side(1, 1)
        hop(1, 2, (1,))
        side(1, 2)
        hop(2, 1, (1,), False)
        hop(2, 1, (0,), True)

    apart(outer, (end_start,))
    apart(middle, (middle_start,))
    for level in range(layers):
        first, second = 2 * level, 2 * level + 1
        last = level == layers - 1
        targets = [target_of(turn_index) for turn_index in range(n_tp)]
        if level > 0:
            contribute(level, targets[2], 0)
            contribute(level, targets[0], 0)
            pass_on(level, targets[2], 0)
            contribute(level, targets[1], 0)
            pass_on(level, targets[0], 0)
            apart(outer, (hop, first, 3, (0,)), (hop, second, 1), (turn, second))
            apart(middle, (hop, second, 1, (0, 1), True))
            contribute(level, targets[0], 1)
            pass_on(level, targets[1], 0)
            apart(middle, (side, first, nz - 2), (hop, second, 1, (0, 1), False))
            contribute(level, targets[2], 1)
            pass_on(level, targets[0], 1)
            contribute(level, targets[1], 1)
            pass_on(level, targets[2], 1)
            apart(middle, (side, second, 1))
            pass_on(level, targets[1], 1)
            apart(outer, (hop, first, 3, (1,)))
            contribute(level, targets[3], 0)
            apart(middle, (own_rows, second), (hop, second, 2))
            pass_on(level, targets[3], 0)
            apart(outer, (side, first, nz - 1))
            contribute(level, targets[3], 1)
            pass_on(level, targets[3], 1)
            apart(middle, (side, second, 2))
            row_scales(level)
            gating(level, y)
            for third in order[:-1]:
                convolve(level, y, third)
            apart(outer, (hop, second, 2))
            gate(level, 1 - y, order[0])
            for index in range(1, tiles):
                gate(level, 1 - y, order[index])
                convolve(level, 1 - y, order[index - 1])
                normalise(level, order[index - 1])
                if index == 1:
                    apart(outer, (hop, second, 3, (0,)))
        for block in (y, 1 - y):
            first_rows(level, block)
            convolve(level, block, order[-1])
        normalise(level, order[-1])
        relay(level, order[0])
        if level > 0:
            apart(outer, (hop, second, 3, (1,)), (side, second, nz - 1))
        else:
            apart(outer, (guest_left,), (side, second, nz - 1))
        for source in range(nz):
            crossed(second, source)
        if not last:
            apart(middle, (hop, first + 2, 1, (1,), True))
        for index in range(1, tiles):
            relay(level, order[index])
            projecting(level, order[index - 1])
            if not last and index == 1:
                apart(middle, (hop, first + 2, 2, (0,)))
                apart(outer, (hop, first + 2, 2, (1,)))
            if not last and index == 2:
                apart(middle, (side, first + 2, 1))
        projecting(level, order[-1])
        if not last:
            for copy in square_copies(level + 1):
                copy.start()
            apart(middle, (hop, first + 2, 2, (1,)))
        settle(level)
    guest_settle()
    for phase in range(len(phases)):
        sent(phase)
    for third in order:
        result_copy(third).wait()


def fused(n_sp, n_tp, *arrays):
    hidden_in, norm_gain, value_proj = arrays[:3]
    rows, feats = hidden_in.shape
    layers = norm_gain.shape[0]
    piece = value_proj.shape[2]
    blocks = n_sp // n_tp
    channels = blocks * piece
    kinds = 4
    tiles = rows // ROW_TILE
    vmem = pl.BlockSpec(memory_space=pltpu.VMEM)
    hbm = pl.BlockSpec(memory_space=pltpu.HBM)
    low, wide = jnp.bfloat16, jnp.float32
    slots = layers * blocks + 3 * (blocks + 1) * (rows // ROW_TILE)
    arrays = arrays[:4] + (arrays[4].transpose(1, 0, 2),) + arrays[5:]
    return pl.pallas_call(
        lambda *refs: fused_kernel(n_sp, n_tp, *refs),
        out_shape=jax.ShapeDtypeStruct((rows, feats), low),
        in_specs=[hbm, vmem, hbm, hbm, vmem, vmem, vmem, vmem, hbm],
        out_specs=hbm,
        scratch_shapes=[
            pltpu.VMEM((rows, feats), low),
            pltpu.VMEM((layers, n_sp, feats, 2 * piece), low),
            pltpu.VMEM((layers, n_sp * piece, feats), low),
            pltpu.VMEM((rows, feats), low),
            pltpu.VMEM((n_tp, blocks, rows, 2 * piece), low),
            pltpu.VMEM((layers, 2, blocks, rows, 2 * piece), low),
            pltpu.VMEM((blocks, rows, 2 * piece), low),
            pltpu.VMEM((layers, blocks, rows, 2 * piece), low),
            pltpu.VMEM((layers, blocks, WIDTH + 1, piece), wide),
            pltpu.VMEM((blocks, HALO + rows, piece), wide),
            pltpu.VMEM((blocks, HALO, piece), low),
            pltpu.VMEM((layers, blocks, HALO, piece), low),
            pltpu.VMEM((blocks, rows, piece), wide),
            pltpu.VMEM((layers, n_tp, rows, channels), low),
            pltpu.VMEM((layers, n_tp, 8, rows), wide),
            pltpu.VMEM((rows, 8), wide),
            pltpu.VMEM((rows, feats), low),
            pltpu.VMEM((2, tiles, blocks, ROW_TILE, 2 * piece), low),
            pltpu.VMEM((tiles, blocks, ROW_TILE, 2 * piece), low),
            pltpu.VMEM((tiles, blocks, ROW_TILE, 2 * piece), low),
            pltpu.VMEM((tiles, blocks, ROW_TILE, 2 * piece), low),
            pltpu.VMEM((tiles, blocks, ROW_TILE, piece), low),
            pltpu.VMEM((tiles, blocks, ROW_TILE, piece), low),
            pltpu.VMEM((8, rows), wide),
            pltpu.VMEM((8, rows), wide),
            pltpu.VMEM((rows, 8), wide),
            pltpu.SemaphoreType.DMA((layers, kinds)),
            pltpu.SemaphoreType.DMA((rows // ROW_TILE,)),
            pltpu.SemaphoreType.DMA((layers * 2, 2 * n_sp + 4)),
            pltpu.SemaphoreType.DMA((layers * 2, 2, n_sp)),
            pltpu.SemaphoreType.DMA((slots,)),
            pltpu.SemaphoreType.DMA((slots,)),
            pltpu.SemaphoreType.DMA((3,)),
            pltpu.SemaphoreType.DMA((3,)),
            pltpu.SemaphoreType.DMA((4 * tiles + 1,)),
            pltpu.SemaphoreType.DMA((4 * tiles + 1,)),
        ],
        compiler_params=pltpu.CompilerParams(
            collective_id=0, has_side_effects=True, vmem_limit_bytes=VMEM_BYTES
        ),
    )(*arrays)


def solution(mesh):
    n_sp, n_tp = mesh.shape["sp"], mesh.shape["tp"]
    piece = C // n_sp
    small = n_tp == 4 and GROUPS == n_tp and n_sp == 8 and piece % 128 == 0

    def local(*arrays):
        if small and arrays[0].shape[0] % ROW_TILE == 0:
            return fused(n_sp, n_tp, *arrays)
        return on_device(*arrays)

    return jax.shard_map(
        local,
        mesh=mesh,
        in_specs=(
            P("sp", "tp"),
            P(None, "tp"),
            P(None, "tp", "sp"),
            P(None, "tp", "sp"),
            P(None, None, "tp"),
            P(None, "tp"),
            P(None, "tp"),
            P(None, "tp"),
            P(None, "sp", "tp"),
        ),
        out_specs=P("sp", "tp"),
        check_vma=False,
    )
```
